256 devices in a mesh: rep: 2 (over z_hi), fs: 16 (over z_lo, x), tp: 8 (over y, core).
Axes of the slice: x: 4, y: 4, z: 8 (z_hi: 2, z_lo: 4; z = z_hi * 4 + z_lo), core: 2. Of those that a mesh axis runs over, the one named last changes fastest.
Arguments:
- tokens: bfloat16 [24576, 2048], P(('rep', 'fs'), 'tp'), may hold values from -6 to 6
- gain_mix: bfloat16 [2048], replicated, may hold values from 0.099609375 to 1.8984375
- query_weight: bfloat16 [2048, 1024], P('fs', 'tp'), may hold values from -0.125 to 0.125
- key_weight: bfloat16 [2048, 1024], P('fs', 'tp'), may hold values from -0.125 to 0.125
- value_weight: bfloat16 [2048, 2048], P('fs', 'tp'), may hold values from -0.125 to 0.125
- gate_weight: bfloat16 [2048, 2048], P('fs', 'tp'), may hold values from -0.125 to 0.125
- decay_rate: float32 [8], P('tp'), may hold values from 0.0006510417 to 0.05
- out_weight: bfloat16 [2048, 2048], P('tp', 'fs'), may hold values from -0.125 to 0.125
- gain_mlp: bfloat16 [2048], replicated, may hold values from 0.099609375 to 1.8984375
- up_weight: bfloat16 [2048, 8192], P('fs', 'tp'), may hold values from -0.125 to 0.125
- down_weight: bfloat16 [8192, 2048], P('tp', 'fs'), may hold values from -0.0625 to 0.0625
Outputs:
- layer_out: bfloat16 [24576, 2048], P(('rep', 'fs'), 'tp')
The draws below stay inside these ranges and needn't reach their ends.
All inputs are finite; a program needn't handle non-finite values.
Results may differ from the reference program's by a relative error of at most 0.019.
Values may be sent and summed in bfloat16 or wider, within the bound.
A program may use at most 128 MiB of HBM per device.

```python
import math
import jax
import jax.numpy as jnp
from jax import lax

D = 2048
HEADS = 8
DK = 128
DV = 256
FF = 8192
SEQ = 768
BLK = 128
TOKENS = 24576
N_TP = 8


def steps_of(rng, shape, pieces, low, top_value):
    level, own = 1.0, jax.random.fold_in(rng, 6)
    for dim, shards_of in pieces:
        heights = jnp.exp(jax.random.uniform(jax.random.fold_in(own, dim), (shards_of,), jnp.float32, low / len(pieces), top_value / len(pieces)))
        level = level * jnp.repeat(heights, shape[dim] // shards_of).reshape([-1 if axis == dim else 1 for axis in range(len(shape))])
    return level


def centred(own_key, dims, spread, bound, split=(), held_as=jnp.bfloat16):
    entries = spread * jax.random.normal(own_key, dims, jnp.float32)
    if split:
        entries = entries * steps_of(own_key, dims, split, -0.22, 0.18)
    return jnp.clip(entries, -bound, bound).astype(held_as)


def setup_inputs(seed: int = 0) -> dict:
    key_list = jax.random.split(jax.random.key(seed), 12)
    tokens = centred(key_list[0], (TOKENS, D), 1.0, 6.0, ((0, 32), (1, 8)))
    gain_mix = jnp.clip(1.0 + 0.18 * jax.random.normal(key_list[1], (D,), jnp.float32), 0.099609375, 1.8984375).astype(jnp.bfloat16)
    query_weight = centred(key_list[2], (D, HEADS * DK), D ** -0.5, 0.125, ((0, 16), (1, 8)))
    key_weight = centred(key_list[3], (D, HEADS * DK), D ** -0.5, 0.125, ((0, 16), (1, 8)))
    value_weight = centred(key_list[4], (D, HEADS * DV), D ** -0.5, 0.125, ((0, 16), (1, 8)))
    gate_weight = centred(key_list[5], (D, HEADS * DV), D ** -0.5, 0.125, ((0, 16), (1, 8)))
    decay_rate = jnp.clip(jnp.exp(math.log(0.05) - 4.3412046 * jax.random.uniform(key_list[6], (HEADS,), jnp.float32) ** steps_of(key_list[6], (HEADS,), ((0, 8),), -0.2, 0.2)), 0.0006510417, 0.05)
    out_weight = centred(key_list[7], (HEADS * DV, D), (HEADS * DV) ** -0.5, 0.125, ((0, 8), (1, 16)))
    gain_mlp = jnp.clip(1.0 + 0.18 * jax.random.normal(key_list[8], (D,), jnp.float32), 0.099609375, 1.8984375).astype(jnp.bfloat16)
    up_weight = centred(key_list[9], (D, FF), D ** -0.5, 0.125, ((0, 16), (1, 8)))
    down_weight = centred(key_list[10], (FF, D), FF ** -0.5, 0.0625, ((0, 8), (1, 16)))
    return dict(tokens=tokens, gain_mix=gain_mix, query_weight=query_weight, key_weight=key_weight, value_weight=value_weight, gate_weight=gate_weight, decay_rate=decay_rate, out_weight=out_weight, gain_mlp=gain_mlp, up_weight=up_weight, down_weight=down_weight)


epsilon = 1e-06
highest = lax.Precision.HIGHEST

def rms_rows(rows, gain):
    values = rows.astype(jnp.float32)
    scaled = values * lax.rsqrt(lax.optimization_barrier(jnp.mean(values * values, axis=-1, keepdims=True)) + epsilon)
    return (scaled * gain.astype(jnp.float32)).astype(jnp.bfloat16)

def retain(query, keys, values, rate, block):
    length, head_count, key_width = query.shape
    value_width = values.shape[-1]
    block_count = length // block
    log_decay = -rate.astype(jnp.float32)
    positions = jnp.arange(block, dtype=jnp.float32)
    distance = positions[:, None] - positions[None, :]
    causal = distance >= 0
    inside = jnp.where(causal[None], jnp.exp(log_decay[:, None, None] * jnp.where(causal, distance, 0.0)[None]), 0.0)
    key_scale = jnp.exp(log_decay[None, :] * (block - 1.0 - positions)[:, None])
    query_scale = jnp.exp(log_decay[None, :] * (positions + 1.0)[:, None])
    carry_decay = jnp.exp(log_decay * block)
    query_blocks = query.reshape(block_count, block, head_count, key_width)
    key_blocks = keys.reshape(block_count, block, head_count, key_width) * key_width ** (-0.5)
    value_blocks = values.reshape(block_count, block, head_count, value_width)

    def advance(state, blocks):
        q_block, k_block, v_block = blocks
        scores = jnp.einsum('ihd,jhd->hij', q_block, k_block, precision=highest) * inside
        inner = jnp.einsum('hij,jhe->ihe', scores, v_block, precision=highest)
        cross = jnp.einsum('ihd,hde->ihe', q_block, state, precision=highest) * query_scale[:, :, None]
        update = jnp.einsum('jhd,jhe->hde', k_block * key_scale[:, :, None], v_block, precision=highest)
        return (state * carry_decay[:, None, None] + update, inner + cross)
    initial = jnp.zeros((head_count, key_width, value_width), jnp.float32)
    _, results = lax.scan(advance, initial, (query_blocks, key_blocks, value_blocks))
    return results.reshape(length, head_count, value_width)

def gated_heads(retained, gate):
    length, head_count, value_width = retained.shape
    normed = retained * lax.rsqrt(lax.optimization_barrier(jnp.mean(retained * retained, axis=-1, keepdims=True)) + epsilon)
    gated = jax.nn.silu(gate.reshape(length, head_count, value_width)) * normed
    return gated.reshape(length, head_count * value_width).astype(jnp.bfloat16)

def grouped_sum(left, right, groups):
    rows = left.shape[0]
    inner_width = left.shape[1] // groups
    left_groups = left.reshape(rows, groups, inner_width).astype(jnp.float32)
    right_groups = right.reshape(groups, inner_width, right.shape[1]).astype(jnp.float32)
    parts = jnp.einsum('sgc,gcd->gsd', left_groups, right_groups)
    rounded = lax.optimization_barrier(parts.astype(jnp.bfloat16)).astype(jnp.float32)
    return lax.optimization_barrier(jnp.sum(rounded, axis=0))

def reference(tokens, gain_mix, query_weight, key_weight, value_weight, gate_weight, decay_rate, out_weight, gain_mlp, up_weight, down_weight):

    def one_sequence(rows):
        normed = rms_rows(rows, gain_mix)
        query = jnp.dot(normed, query_weight, preferred_element_type=jnp.float32).reshape(SEQ, HEADS, DK)
        keys = jnp.dot(normed, key_weight, preferred_element_type=jnp.float32).reshape(SEQ, HEADS, DK)
        values = jnp.dot(normed, value_weight, preferred_element_type=jnp.float32).reshape(SEQ, HEADS, DV)
        gate = jnp.dot(normed, gate_weight, preferred_element_type=jnp.float32)
        retained = retain(query, keys, values, decay_rate, BLK)
        hidden = gated_heads(retained, gate)
        mixed = (rows.astype(jnp.float32) + grouped_sum(hidden, out_weight, N_TP)).astype(jnp.bfloat16)
        normed_mlp = rms_rows(mixed, gain_mlp)
        upward = jnp.dot(normed_mlp, up_weight, preferred_element_type=jnp.float32)
        active = jnp.square(jax.nn.relu(upward)).astype(jnp.bfloat16)
        return (mixed.astype(jnp.float32) + grouped_sum(active, down_weight, N_TP)).astype(jnp.bfloat16)
    sequences = tokens.reshape(TOKENS // SEQ, SEQ, D)
    return lax.map(one_sequence, sequences).reshape(TOKENS, D)
```

```python
import functools

import jax
import jax.numpy as jnp
from jax import lax
from jax.experimental import pallas as pl
from jax.experimental.pallas import tpu as pltpu
from jax.sharding import Mesh
from jax.sharding import PartitionSpec as P

DK = 128
DV = 256
SEQ = 768
D = 2048
CH = 256
NCH = SEQ // CH
HC = CH // 2
EPS = 1e-06
F32 = jnp.float32
BF16 = jnp.bfloat16
TP = ("y", "c")
FS = ("zl", "x")
MESH_ID = pl.DeviceIdType.MESH
N_REMOTE = 160
N_LOCAL = 16


def kernel(
    tok, gmix, qw, kw, vw, gw, rate, ow, gmlp, uw, dw,
    out,
    xg, mg, nrm, wq, wo, wu, wd, kbuf, vbuf, dec, own, snd, prc,
    s_a, s_b, s_p, s_m, r_a, r_b, r_p, r_m, outv,
    send_sem, recv_sem, local_sem,
):
    rep, zl = lax.axis_index("rep"), lax.axis_index("zl")
    x, y, c = lax.axis_index("x"), lax.axis_index("y"), lax.axis_index("c")

    def mod4(v):
        return lax.rem(v + 4, 4)

    def z_id(step):
        z = lax.rem(rep * 4 + zl + step + 8, 8)
        return {"rep": z // 4, "zl": lax.rem(z, 4)}

    xp, xm, x2 = mod4(x + 1), mod4(x - 1), mod4(x + 2)
    zp, zm, z2 = mod4(zl + 1), mod4(zl - 1), mod4(zl + 2)
    yp, ym, y2 = mod4(y + 1), mod4(y - 1), mod4(y + 2)
    to_xp, to_xm = {"x": xp}, {"x": xm}
    to_zp, to_zm = z_id(1), z_id(-1)
    to_yp, to_ym = {"y": yp}, {"y": ym}
    to_pair = {"c": 1 - c}

    ids = {}

    def remote(name, src, dst, dev):
        i = ids.setdefault(name, len(ids))
        return pltpu.make_async_remote_copy(
            src_ref=src,
            dst_ref=dst,
            send_sem=send_sem.at[i],
            recv_sem=recv_sem.at[i],
            device_id=dev,
            device_id_type=MESH_ID,
        )

    sent = []

    def send(name, src, dst, dev):
        copy = remote(name, src, dst, dev)
        copy.start()
        sent.append(copy)

    def arrived(name, dst, dev):
        remote(name, dst, dst, dev).wait_recv()

    local_ids = {}

    def local(name, src, dst):
        i = local_ids.setdefault(name, len(local_ids))
        return pltpu.make_async_copy(src, dst, local_sem.at[i])

    me = y * 2 + c
    wq_own = wq.at[zl, x]
    loads = {
        "tok": local("tok", tok, xg.at[me]),
        "q": local("q", qw, wq_own.at[:, pl.ds(0, DK)]),
        "k": local("k", kw, wq_own.at[:, pl.ds(DK, DK)]),
        "v": local("v", vw, wq_own.at[:, pl.ds(2 * DK, DV)]),
        "g": local("g", gw, wq_own.at[:, pl.ds(2 * DK + DV, DV)]),
        "o": local("o", ow, wo.at[zl, x]),
        "u": local("u", uw, wu.at[zl, x]),
        "d": local("d", dw, wd.at[zl, x]),
    }
    for load in loads.values():
        load.start()

    barrier = pltpu.get_barrier_semaphore()
    for dev in (to_xp, to_xm, to_zp, to_zm, to_yp, to_ym, to_pair):
        pl.semaphore_signal(barrier, inc=1, device_id=dev, device_id_type=MESH_ID)
    pl.semaphore_wait(barrier, 7)

    weights = {"q": (wq, 128), "o": (wo, 256), "u": (wu, 128), "d": (wd, 1024)}

    def rows_of(w, half, quarter=None):
        n = weights[w][1] // 2
        start = 0 if half == "A" else n
        if quarter is None:
            return pl.ds(start, n)
        return pl.ds(start + quarter * (n // 2), n // 2)

    def first_slab(w, half, at, quarter=None):
        buf = weights[w][0]
        rows = rows_of(w, half, quarter)
        return buf.at[zl, at, rows] if half == "A" else buf.at[at, x, rows]

    def second_slab(w, half, at, quarter=None):
        buf = weights[w][0]
        rows = rows_of(w, half, quarter)
        return buf.at[at, :, rows] if half == "A" else buf.at[:, at, rows]

    ring_x = (x, xp, xm, x2, to_xp, to_xm)
    ring_z = (zl, zp, zm, z2, to_zp, to_zm)

    def rings(half):
        return (ring_x, ring_z) if half == "A" else (ring_z, ring_x)

    def w1(w):
        for half in "AB":
            (at, _, _, _, plus, minus), _ = rings(half)
            slab = first_slab(w, half, at)
            send((w, half, "1p"), slab, slab, plus)
            send((w, half, "1m"), slab, slab, minus)

    def w2(w):
        for half in "AB":
            (_, up, dn, _, plus, minus), _ = rings(half)
            arrived((w, half, "1p"), first_slab(w, half, dn), plus)
            slab = first_slab(w, half, dn, 0)
            send((w, half, "2p"), slab, slab, plus)
            arrived((w, half, "1m"), first_slab(w, half, up), minus)
            slab = first_slab(w, half, up, 1)
            send((w, half, "2m"), slab, slab, minus)

    def w3(w):
        for half in "AB":
            (_, _, _, far, plus, minus), (at, _, _, _, plus2, minus2) = rings(half)
            arrived((w, half, "2p"), first_slab(w, half, far, 0), plus)
            arrived((w, half, "2m"), first_slab(w, half, far, 1), minus)
            slab = second_slab(w, half, at)
            send((w, half, "3p"), slab, slab, plus2)
            send((w, half, "3m"), slab, slab, minus2)

    def w4(w):
        for half in "AB":
            _, (_, up, dn, _, plus, minus) = rings(half)
            arrived((w, half, "3p"), second_slab(w, half, dn), plus)
            slab = second_slab(w, half, dn, 0)
            send((w, half, "4p"), slab, slab, plus)
            arrived((w, half, "3m"), second_slab(w, half, up), minus)
            slab = second_slab(w, half, up, 1)
            send((w, half, "4m"), slab, slab, minus)

    def w5(w):
        for half in "AB":
            _, (_, _, _, far, plus, minus) = rings(half)
            arrived((w, half, "4p"), second_slab(w, half, far, 0), plus)
            arrived((w, half, "4m"), second_slab(w, half, far, 1), minus)

    blk = lambda yy, cc: yy * 2 + cc
    other = 1 - c

    def part(buf, b, r, half=None):
        if half is None:
            return buf.at[b, pl.ds(r * CH, CH)]
        return buf.at[b, pl.ds(r * CH + half * HC, HC)]

    def g1(tag, buf, r):
        s = part(buf, blk(y, c), r)
        send((tag, r, "1p"), s, s, to_yp)
        send((tag, r, "1m"), s, s, to_ym)
        send((tag, r, "c0"), s, s, to_pair)

    def g2(tag, buf, r):
        arrived((tag, r, "1p"), part(buf, blk(ym, c), r), to_yp)
        s = part(buf, blk(ym, c), r, 0)
        send((tag, r, "2p"), s, s, to_yp)
        arrived((tag, r, "1m"), part(buf, blk(yp, c), r), to_ym)
        s = part(buf, blk(yp, c), r, 1)
        send((tag, r, "2m"), s, s, to_ym)
        s = part(buf, blk(ym, c), r)
        send((tag, r, "c1"), s, s, to_pair)
        s = part(buf, blk(yp, c), r)
        send((tag, r, "c2"), s, s, to_pair)

    def g3(tag, buf, r):
        s = part(buf, blk(y2, c), r, 0)
        arrived((tag, r, "2p"), s, to_yp)
        send((tag, r, "c3"), s, s, to_pair)
        s = part(buf, blk(y2, c), r, 1)
        arrived((tag, r, "2m"), s, to_ym)
        send((tag, r, "c4"), s, s, to_pair)

    def g4(tag, buf, r):
        arrived((tag, r, "c0"), part(buf, blk(y, other), r), to_pair)
        arrived((tag, r, "c1"), part(buf, blk(ym, other), r), to_pair)
        arrived((tag, r, "c2"), part(buf, blk(yp, other), r), to_pair)
        arrived((tag, r, "c3"), part(buf, blk(y2, other), r, 0), to_pair)
        arrived((tag, r, "c4"), part(buf, blk(y2, other), r, 1), to_pair)

    def rows(r):
        return pl.ds(r * CH, CH)

    def s0(p, r):
        s = snd.at[p, :, rows(r)]
        send(("s", p, r, "0"), s, prc.at[p, :, rows(r)], to_pair)

    def pair_sum(p, r, b, lo, n):
        at = pl.ds(r * CH + lo, n)
        return own[p, b, at, :].astype(F32) + prc[p, b, at, :].astype(F32)

    def s1(p, r):
        arrived(("s", p, r, "0"), prc.at[p, :, rows(r)], to_pair)
        s_a[p, r] = pair_sum(p, r, y2, 0, HC).astype(BF16)
        send(("s", p, r, "1p"), s_a.at[p, r], r_a.at[p, r], to_yp)
        s_b[p, r] = pair_sum(p, r, y2, HC, HC).astype(BF16)
        send(("s", p, r, "1m"), s_b.at[p, r], r_b.at[p, r], to_ym)

    def s2(p, r):
        s_p[p, r, pl.ds(HC, HC)] = pair_sum(p, r, yp, HC, HC).astype(BF16)
        s_m[p, r, pl.ds(0, HC)] = pair_sum(p, r, ym, 0, HC).astype(BF16)
        arrived(("s", p, r, "1p"), r_a.at[p, r], to_yp)
        s_p[p, r, pl.ds(0, HC)] = (
            pair_sum(p, r, yp, 0, HC) + r_a[p, r].astype(F32)
        ).astype(BF16)
        send(("s", p, r, "2p"), s_p.at[p, r], r_p.at[p, r], to_yp)
        arrived(("s", p, r, "1m"), r_b.at[p, r], to_ym)
        s_m[p, r, pl.ds(HC, HC)] = (
            pair_sum(p, r, ym, HC, HC) + r_b[p, r].astype(F32)
        ).astype(BF16)
        send(("s", p, r, "2m"), s_m.at[p, r], r_m.at[p, r], to_ym)

    def s3(p, r):
        total = pair_sum(p, r, y, 0, CH)
        arrived(("s", p, r, "2p"), r_p.at[p, r], to_yp)
        arrived(("s", p, r, "2m"), r_m.at[p, r], to_ym)
        total = total + (r_p[p, r].astype(F32) + r_m[p, r].astype(F32))
        if p == 0:
            mg[me, rows(r), :] = (xg[me, rows(r), :].astype(F32) + total).astype(BF16)
        else:
            outv[rows(r), :] = (mg[me, rows(r), :].astype(F32) + total).astype(BF16)

    def norm(src, gain, r):
        def body(i, carry):
            at = pl.ds(pl.multiple_of(r * CH + i * 64, 64), 64)
            square = jnp.zeros((64, DV), F32)
            for b in range(8):
                v = src[b, at, :].astype(F32)
                square = square + v * v
            mean = jnp.sum(square, axis=-1, keepdims=True) * (1.0 / D)
            scale = lax.rsqrt(mean + EPS)
            for b in range(8):
                v = src[b, at, :].astype(F32)
                g = gain[b : b + 1, :].astype(F32)
                nrm[at, b * DV : (b + 1) * DV] = (v * scale * g).astype(BF16)
            return carry

        lax.fori_loop(0, CH // 64, body, 0, unroll=2)

    def decays():
        rt = rate[0]
        i = lax.broadcasted_iota(jnp.int32, (CH, CH), 0)
        j = lax.broadcasted_iota(jnp.int32, (CH, CH), 1)
        near = (i - j).astype(F32)
        for d in range(NCH):
            dist = near + float(d * CH)
            value = jnp.exp(-rt * jnp.maximum(dist, 0.0)) * DK ** (-0.5)
            dec[d] = jnp.where(dist >= 0.0, value, 0.0)

    def dot(a, b):
        return jnp.dot(a, b, preferred_element_type=F32)

    def scatter_parts(p, r, left, w):
        for b in range(4):
            for dst, cc in ((snd, other), (own, c)):
                right = jnp.concatenate([w[b, 2 * cc], w[b, 2 * cc + 1]], axis=1)
                dst[p, b, rows(r), :] = dot(left, right).astype(BF16)

    def mix(r):
        a = nrm[rows(r), :]
        qkv = dot(a, wq[:, :, :, 0 : 2 * DK + DV].reshape(D, 2 * DK + DV))
        q = qkv[:, :DK].astype(BF16)
        kbuf[rows(r), :] = qkv[:, DK : 2 * DK].astype(BF16)
        vbuf[rows(r), :] = qkv[:, 2 * DK :].astype(BF16)
        gate = dot(a, wq[:, :, :, 2 * DK + DV :].reshape(D, DV))
        kept = jnp.zeros((CH, DV), F32)
        for b in range(r + 1):
            score = lax.dot_general(
                q, kbuf[rows(b), :], (((1,), (1,)), ((), ())), preferred_element_type=F32
            )
            score = (score * dec[r - b]).astype(BF16)
            kept = kept + dot(score, vbuf[rows(b), :])
        mean = jnp.mean(kept * kept, axis=-1, keepdims=True)
        kept = kept * lax.rsqrt(mean + EPS)
        hidden = (gate / (1.0 + jnp.exp(-gate)) * kept).astype(BF16)
        scatter_parts(0, r, hidden, wo)

    def mlp_up(r):
        a = nrm[rows(r), :]
        active = []
        for b in range(4):
            upward = dot(a, wu[:, :, :, b * 256 : (b + 1) * 256].reshape(D, 256))
            upward = jnp.maximum(upward, 0.0)
            active.append((upward * upward).astype(BF16))
        return jnp.concatenate(active, axis=1)

    loads["tok"].wait()
    for r in range(NCH):
        g1("t", xg, r)
    for name in "qkvg":
        loads[name].wait()
    w1("q")
    loads["o"].wait()
    w1("o")
    decays()
    w2("q")
    g2("t", xg, 0)
    loads["u"].wait()
    loads["d"].wait()
    w3("q")
    w2("o")
    g2("t", xg, 1)
    w1("u")
    w3("o")
    g2("t", xg, 2)
    for r in range(NCH):
        g3("t", xg, r)
    w1("d")
    w4("q")
    w2("u")
    w4("o")
    for r in range(NCH):
        g4("t", xg, r)
        norm(xg, gmix, r)
    w3("u")
    w2("d")
    w5("q")
    w5("o")
    mix(0)
    s0(0, 0)
    w3("d")
    mix(1)
    s0(0, 1)
    s1(0, 0)
    mix(2)
    s0(0, 2)
    s2(0, 0)
    s1(0, 1)
    w4("u")
    s1(0, 2)
    s2(0, 1)
    s3(0, 0)
    g1("m", mg, 0)
    s2(0, 2)
    s3(0, 1)
    g1("m", mg, 1)
    g2("m", mg, 0)
    s3(0, 2)
    g1("m", mg, 2)
    g2("m", mg, 1)
    g3("m", mg, 0)
    g2("m", mg, 2)
    g3("m", mg, 1)
    w4("d")
    g4("m", mg, 0)
    norm(mg, gmlp, 0)
    w5("u")
    g3("m", mg, 2)
    active = [mlp_up(0)]
    g4("m", mg, 1)
    norm(mg, gmlp, 1)
    active.append(mlp_up(1))
    g4("m", mg, 2)
    norm(mg, gmlp, 2)
    active.append(mlp_up(2))
    w5("d")
    scatter_parts(1, 0, active[0], wd)
    s0(1, 0)
    scatter_parts(1, 1, active[1], wd)
    s0(1, 1)
    s1(1, 0)
    scatter_parts(1, 2, active[2], wd)
    s0(1, 2)
    s1(1, 1)
    s2(1, 0)
    s1(1, 2)
    s2(1, 1)
    s3(1, 0)
    stores = []
    s2(1, 2)
    s3(1, 1)
    s3(1, 2)
    store = local("out", outv, out)
    store.start()
    for copy in sent:
        copy.wait_send()
    store.wait()


def local(
    tokens, gain_mix, query_weight, key_weight, value_weight, gate_weight,
    decay_rate, out_weight, gain_mlp, up_weight, down_weight,
):
    hbm = pl.BlockSpec(memory_space=pl.ANY)
    vmem = pl.BlockSpec(memory_space=pltpu.VMEM)
    smem = pl.BlockSpec(memory_space=pltpu.SMEM)
    half = lambda n, w: pltpu.VMEM((2, NCH, n, w), BF16)
    return pl.pallas_call(
        kernel,
        out_shape=jax.ShapeDtypeStruct((SEQ, DV), BF16),
        in_specs=[hbm, vmem, hbm, hbm, hbm, hbm, smem, hbm, vmem, hbm, hbm],
        out_specs=hbm,
        scratch_shapes=[
            pltpu.VMEM((8, SEQ, DV), BF16),
            pltpu.VMEM((8, SEQ, DV), BF16),
            pltpu.VMEM((SEQ, D), BF16),
            pltpu.VMEM((4, 4, 128, 768), BF16),
            pltpu.VMEM((4, 4, 256, 128), BF16),
            pltpu.VMEM((4, 4, 128, 1024), BF16),
            pltpu.VMEM((4, 4, 1024, 128), BF16),
            pltpu.VMEM((SEQ, DK), BF16),
            pltpu.VMEM((SEQ, DV), BF16),
            pltpu.VMEM((NCH, CH, CH), F32),
            pltpu.VMEM((2, 4, SEQ, DV), BF16),
            pltpu.VMEM((2, 4, SEQ, DV), BF16),
            pltpu.VMEM((2, 4, SEQ, DV), BF16),
            half(HC, DV), half(HC, DV), half(CH, DV), half(CH, DV),
            half(HC, DV), half(HC, DV), half(CH, DV), half(CH, DV),
            pltpu.VMEM((SEQ, DV), BF16),
            pltpu.SemaphoreType.DMA((N_REMOTE,)),
            pltpu.SemaphoreType.DMA((N_REMOTE,)),
            pltpu.SemaphoreType.DMA((N_LOCAL,)),
        ],
        compiler_params=pltpu.CompilerParams(
            collective_id=0, has_side_effects=True, vmem_limit_bytes=62 * 1024 * 1024
        ),
    )(
        tokens, gain_mix.reshape(8, DV), query_weight, key_weight, value_weight, gate_weight,
        decay_rate, out_weight, gain_mlp.reshape(8, DV), up_weight, down_weight,
    )


def solution(mesh):
    finer = Mesh(
        mesh.devices.reshape(mesh.shape["rep"], 4, 4, 4, 2), ("rep", "zl", "x", "y", "c")
    )
    placed = (
        P(("rep", "zl", "x"), TP), P(), P(FS, TP), P(FS, TP), P(FS, TP), P(FS, TP),
        P(TP), P(TP, FS), P(), P(FS, TP), P(TP, FS),
    )
    return jax.shard_map(
        local, mesh=finer, in_specs=placed, out_specs=P(("rep", "zl", "x"), TP), check_vma=False
    )
```

```python
import functools

import jax
import jax.numpy as jnp
from jax import lax
from jax.experimental import pallas as pl
from jax.experimental.pallas import tpu as pltpu
from jax.sharding import Mesh
from jax.sharding import PartitionSpec as P

DK = 128
DV = 256
SEQ = 768
D = 2048
CH = 256
NCH = SEQ // CH
HC = CH // 2
EPS = 1e-06
F32 = jnp.float32
BF16 = jnp.bfloat16
TP = ("y", "c")
FS = ("zl", "x")
ORDER = [
    ('load', 't'), ('load', 'o'), ('load', 'ud'), ('w1', 'o', 'B'), ('w1', 'o', 'A'), ('load', 'qkvg'),
    ('w1', 'q', 'A'), ('g1', 't', 0), ('w1', 'q', 'B'), ('w3o', 'q', 'A'), ('w3o', 'q', 'B'), ('decays',),
    ('w2', 'o', 'B'), ('w3o', 'o', 'B'), ('w2', 'o', 'A'), ('w1', 'u', 'B'), ('w2', 'q', 'A'),
    ('w2', 'q', 'B'), ('w3n', 'q', 'B'), ('w3n', 'o', 'B'), ('g1', 't', 2), ('w3n', 'q', 'A'),
    ('w3o', 'o', 'A'), ('g1', 't', 1), ('w3f', 'o', 'B'), ('g2', 't', 2), ('g2', 't', 0), ('w3f', 'q', 'B'),
    ('w3f', 'q', 'A'), ('w4o', 'q', 'B'), ('w3f', 'o', 'A'), ('w3n', 'o', 'A'), ('g2', 't', 1),
    ('w4n', 'o', 'B'), ('w4n', 'q', 'B'), ('w4n', 'q', 'A'), ('g3', 't', 2), ('w4o', 'o', 'B'),
    ('w4f', 'o', 'B'), ('w4f', 'q', 'B'), ('w4f', 'q', 'A'), ('w4o', 'q', 'A'), ('w5o', 'q', 'B'),
    ('g3', 't', 1), ('w4o', 'o', 'A'), ('w1', 'u', 'A'), ('w4f', 'o', 'A'), ('w4n', 'o', 'A'),
    ('w1', 'd', 'A'), ('g3', 't', 0), ('w2', 'u', 'B'), ('g4', 't', 0), ('g4', 't', 1), ('w5n', 'o', 'B'),
    ('norm', 't', 0), ('w5f', 'o', 'B'), ('g4', 't', 2), ('w5n', 'q', 'A'), ('w1', 'd', 'B'),
    ('norm', 't', 1), ('w3o', 'd', 'A'), ('w5o', 'o', 'B'), ('w3n', 'u', 'B'), ('norm', 't', 2),
    ('w5n', 'q', 'B'), ('w5f', 'q', 'B'), ('w5f', 'q', 'A'), ('w3o', 'u', 'A'), ('w5o', 'q', 'A'),
    ('mixa', 0), ('w5f', 'o', 'A'), ('w5o', 'o', 'A'), ('w5n', 'o', 'A'), ('mix', 0), ('s0', 0, 0),
    ('mixa', 1), ('mix', 1), ('w2', 'u', 'A'), ('s0', 0, 1), ('s1', 0, 0), ('mixa', 2), ('mix', 2),
    ('s0', 0, 2), ('w2', 'd', 'B'), ('w3f', 'u', 'B'), ('s1', 0, 1), ('w3n', 'd', 'B'), ('s1', 0, 2),
    ('s2', 0, 0), ('w2', 'd', 'A'), ('w3o', 'u', 'B'), ('w3n', 'u', 'A'), ('w4n', 'u', 'B'),
    ('w3f', 'u', 'A'), ('w3n', 'd', 'A'), ('w3f', 'd', 'B'), ('s2', 0, 1), ('s2', 0, 2), ('s3', 0, 0),
    ('g1', 'm', 0), ('w4n', 'u', 'A'), ('w4o', 'u', 'A'), ('s3', 0, 1), ('g1', 'm', 1), ('w4o', 'u', 'B'),
    ('s3', 0, 2), ('w4f', 'u', 'B'), ('w4f', 'u', 'A'), ('g1', 'm', 2), ('w3o', 'd', 'B'), ('w4n', 'd', 'A'),
    ('g2', 'm', 1), ('w3f', 'd', 'A'), ('g2', 'm', 0), ('w5n', 'u', 'B'), ('g2', 'm', 2), ('w4o', 'd', 'A'),
    ('w5n', 'u', 'A'), ('w4f', 'd', 'B'), ('g3', 'm', 1), ('w5o', 'u', 'A'), ('w5f', 'u', 'A'),
    ('w4n', 'd', 'B'), ('w5f', 'u', 'B'), ('g3', 'm', 0), ('w5o', 'u', 'B'), ('g4', 'm', 1), ('norm', 'm', 1),
    ('up', 1), ('g4', 'm', 0), ('norm', 'm', 0), ('w5n', 'd', 'A'), ('g3', 'm', 2), ('w4o', 'd', 'B'),
    ('down', 1, 1), ('s0', 1, 1), ('up', 0), ('down', 1, 0), ('s0', 1, 0), ('s1', 1, 1), ('g4', 'm', 2),
    ('w4f', 'd', 'A'), ('norm', 'm', 2), ('up', 2), ('s1', 1, 0), ('down', 1, 2), ('w5n', 'd', 'B'),
    ('s0', 1, 2), ('w5f', 'd', 'B'), ('w5o', 'd', 'A'), ('s2', 1, 1), ('w5o', 'd', 'B'), ('s1', 1, 2),
    ('w5f', 'd', 'A'), ('down', 2, 1), ('s0', 2, 1), ('s2', 1, 0), ('down', 2, 2), ('s0', 2, 2),
    ('down', 2, 0), ('s0', 2, 0), ('s1', 2, 1), ('s1', 2, 2), ('s1', 2, 0), ('s2', 1, 2), ('s3', 1, 0),
    ('s3', 1, 1), ('s2', 2, 1), ('s2', 2, 2), ('s2', 2, 0), ('s3', 1, 2), ('s3', 2, 2), ('s3', 2, 1),
    ('s3', 2, 0),
]
MESH_ID = pl.DeviceIdType.MESH
N_REMOTE = 260
N_LOCAL = 16


def kernel(
    tok, gmix, qw, kw, vw, gw, rate, ow, gmlp, uw, dw,
    out,
    xg, mg, nrm, wq, wo, wu, wd, kbuf, vbuf, dec, hid, act, outv,
    send_sem, recv_sem, local_sem, *summing,
):
    sums = [summing[11 * p : 11 * p + 11] for p in range(3)]
    rep, zl = lax.axis_index("rep"), lax.axis_index("zl")
    x, y, c = lax.axis_index("x"), lax.axis_index("y"), lax.axis_index("c")

    def mod4(v):
        return lax.rem(v + 4, 4)

    def z_id(step):
        z = lax.rem(rep * 4 + zl + step + 8, 8)
        return {"rep": z // 4, "zl": lax.rem(z, 4)}

    xp, xm, x2 = mod4(x + 1), mod4(x - 1), mod4(x + 2)
    zp, zm, z2 = mod4(zl + 1), mod4(zl - 1), mod4(zl + 2)
    yp, ym, y2 = mod4(y + 1), mod4(y - 1), mod4(y + 2)
    to_xp, to_xm = {"x": xp}, {"x": xm}
    to_zp, to_zm = z_id(1), z_id(-1)
    to_yp, to_ym = {"y": yp}, {"y": ym}
    to_pair = {"c": 1 - c}

    ids = {}

    def remote(name, src, dst, dev):
        i = ids.setdefault(name, len(ids))
        return pltpu.make_async_remote_copy(
            src_ref=src,
            dst_ref=dst,
            send_sem=send_sem.at[i],
            recv_sem=recv_sem.at[i],
            device_id=dev,
            device_id_type=MESH_ID,
        )

    sent = []

    def send(name, src, dst, dev):
        copy = remote(name, src, dst, dev)
        copy.start()
        sent.append(copy)

    def arrived(name, dst, dev):
        remote(name, dst, dst, dev).wait_recv()

    local_ids = {}

    def local(name, src, dst):
        i = local_ids.setdefault(name, len(local_ids))
        return pltpu.make_async_copy(src, dst, local_sem.at[i])

    me = y * 2 + c
    wq_own = wq.at[zl, x]
    loads = {
        "t": local("t", tok, xg.at[me]),
        "q": local("q", qw, wq_own.at[:, pl.ds(0, DK)]),
        "k": local("k", kw, wq_own.at[:, pl.ds(DK, DK)]),
        "v": local("v", vw, wq_own.at[:, pl.ds(2 * DK, DV)]),
        "g": local("g", gw, wq_own.at[:, pl.ds(2 * DK + DV, DV)]),
        "o": local("o", ow, wo.at[zl, x]),
        "u": local("u", uw, wu.at[zl, x]),
        "d": local("d", dw, wd.at[zl, x]),
    }
    for load in loads.values():
        load.start()

    barrier = pltpu.get_barrier_semaphore()
    for dev in (to_xp, to_xm, to_zp, to_zm, to_yp, to_ym, to_pair):
        pl.semaphore_signal(barrier, inc=1, device_id=dev, device_id_type=MESH_ID)
    pl.semaphore_wait(barrier, 7)

    weights = {"q": (wq, 128), "o": (wo, 256), "u": (wu, 128), "d": (wd, 1024)}

    def slab(w, half, first, second, quarter=None):
        buf, n = weights[w]
        start, size = (0 if half == "A" else n // 2), n // 2
        if quarter is not None:
            size //= 2
            start += quarter * size
        zi, xi = (second, first) if half == "A" else (first, second)
        return buf.at[zi, xi, pl.ds(start, size)]

    ring_x = (x, xp, xm, x2, to_xp, to_xm)
    ring_z = (zl, zp, zm, z2, to_zp, to_zm)

    def rings(half):
        return (ring_x, ring_z) if half == "A" else (ring_z, ring_x)

    def w1(w, half):
        (at, _, _, _, plus, minus), (here, *_) = rings(half)
        s = slab(w, half, at, here)
        send((w, half, "1p"), s, s, plus)
        send((w, half, "1m"), s, s, minus)

    def w2(w, half):
        (_, up, dn, _, plus, minus), (here, *_) = rings(half)
        arrived((w, half, "1p"), slab(w, half, dn, here), plus)
        s = slab(w, half, dn, here, 0)
        send((w, half, "2p"), s, s, plus)
        arrived((w, half, "1m"), slab(w, half, up, here), minus)
        s = slab(w, half, up, here, 1)
        send((w, half, "2m"), s, s, minus)

    def slabs_of(kind, ring):
        at, up, dn, far, _, _ = ring
        return {"o": [("o", at)], "n": [("u", up), ("d", dn)], "f": [("f", far)]}[kind]

    def w3(kind, w, half):
        first, (here, _, _, _, plus, minus) = rings(half)
        if kind == "f":
            far = first[3]
            arrived((w, half, "2p"), slab(w, half, far, here, 0), first[4])
            arrived((w, half, "2m"), slab(w, half, far, here, 1), first[5])
        for tag, i in slabs_of(kind, first):
            s = slab(w, half, i, here)
            send((w, half, "3p", tag), s, s, plus)
            send((w, half, "3m", tag), s, s, minus)

    def w4(kind, w, half):
        first, (_, up, dn, _, plus, minus) = rings(half)
        for tag, i in slabs_of(kind, first):
            arrived((w, half, "3p", tag), slab(w, half, i, dn), plus)
            s = slab(w, half, i, dn, 0)
            send((w, half, "4p", tag), s, s, plus)
            arrived((w, half, "3m", tag), slab(w, half, i, up), minus)
            s = slab(w, half, i, up, 1)
            send((w, half, "4m", tag), s, s, minus)

    def w5(kind, w, half):
        first, (_, _, _, far, plus, minus) = rings(half)
        for tag, i in slabs_of(kind, first):
            arrived((w, half, "4p", tag), slab(w, half, i, far, 0), plus)
            arrived((w, half, "4m", tag), slab(w, half, i, far, 1), minus)

    blk = lambda yy, cc: yy * 2 + cc
    other = 1 - c

    def part(buf, b, r, half=None):
        if half is None:
            return buf.at[b, pl.ds(r * CH, CH)]
        return buf.at[b, pl.ds(r * CH + half * HC, HC)]

    def g1(tag, buf, r):
        s = part(buf, blk(y, c), r)
        send((tag, r, "1p"), s, s, to_yp)
        send((tag, r, "1m"), s, s, to_ym)
        send((tag, r, "c0"), s, s, to_pair)

    def g2(tag, buf, r):
        arrived((tag, r, "1p"), part(buf, blk(ym, c), r), to_yp)
        s = part(buf, blk(ym, c), r, 0)
        send((tag, r, "2p"), s, s, to_yp)
        arrived((tag, r, "1m"), part(buf, blk(yp, c), r), to_ym)
        s = part(buf, blk(yp, c), r, 1)
        send((tag, r, "2m"), s, s, to_ym)
        s = part(buf, blk(ym, c), r)
        send((tag, r, "c1"), s, s, to_pair)
        s = part(buf, blk(yp, c), r)
        send((tag, r, "c2"), s, s, to_pair)

    def g3(tag, buf, r):
        s = part(buf, blk(y2, c), r, 0)
        arrived((tag, r, "2p"), s, to_yp)
        send((tag, r, "c3"), s, s, to_pair)
        s = part(buf, blk(y2, c), r, 1)
        arrived((tag, r, "2m"), s, to_ym)
        send((tag, r, "c4"), s, s, to_pair)

    def g4(tag, buf, r):
        arrived((tag, r, "c0"), part(buf, blk(y, other), r), to_pair)
        arrived((tag, r, "c1"), part(buf, blk(ym, other), r), to_pair)
        arrived((tag, r, "c2"), part(buf, blk(yp, other), r), to_pair)
        arrived((tag, r, "c3"), part(buf, blk(y2, other), r, 0), to_pair)
        arrived((tag, r, "c4"), part(buf, blk(y2, other), r, 1), to_pair)

    def rows(r):
        return pl.ds(r * CH, CH)

    def s0(p, r):
        own, snd, prc = sums[p][:3]
        send(("s", p, r, "0"), snd.at[:, rows(r)], prc.at[:, rows(r)], to_pair)

    def pair_sum(p, r, b, lo, n):
        own, snd, prc = sums[p][:3]
        at = pl.ds(r * CH + lo, n)
        return own[b, at, :].astype(F32) + prc[b, at, :].astype(F32)

    def s1(p, r):
        _, _, prc, s_a, s_b, _, _, r_a, r_b, _, _ = sums[p]
        arrived(("s", p, r, "0"), prc.at[:, rows(r)], to_pair)
        s_a[r] = pair_sum(p, r, y2, 0, HC).astype(BF16)
        send(("s", p, r, "1p"), s_a.at[r], r_a.at[r], to_yp)
        s_b[r] = pair_sum(p, r, y2, HC, HC).astype(BF16)
        send(("s", p, r, "1m"), s_b.at[r], r_b.at[r], to_ym)

    def s2(p, r):
        _, _, _, _, _, s_p, s_m, r_a, r_b, r_p, r_m = sums[p]
        s_p[r, pl.ds(HC, HC)] = pair_sum(p, r, yp, HC, HC).astype(BF16)
        s_m[r, pl.ds(0, HC)] = pair_sum(p, r, ym, 0, HC).astype(BF16)
        arrived(("s", p, r, "1p"), r_a.at[r], to_yp)
        s_p[r, pl.ds(0, HC)] = (pair_sum(p, r, yp, 0, HC) + r_a[r].astype(F32)).astype(BF16)
        send(("s", p, r, "2p"), s_p.at[r], r_p.at[r], to_yp)
        arrived(("s", p, r, "1m"), r_b.at[r], to_ym)
        s_m[r, pl.ds(HC, HC)] = (pair_sum(p, r, ym, HC, HC) + r_b[r].astype(F32)).astype(BF16)
        send(("s", p, r, "2m"), s_m.at[r], r_m.at[r], to_ym)

    odd = lax.rem(x, 2)
    column = {1: 1 - odd, 2: odd}
    stores = []

    def s3(p, r):
        r_p, r_m = sums[p][9:]
        total = pair_sum(p, r, y, 0, CH)
        arrived(("s", p, r, "2p"), r_p.at[r], to_yp)
        arrived(("s", p, r, "2m"), r_m.at[r], to_ym)
        total = total + (r_p[r].astype(F32) + r_m[r].astype(F32))
        if p == 0:
            mg[me, rows(r), :] = (xg[me, rows(r), :].astype(F32) + total).astype(BF16)
            return
        mixed = mg[me, rows(r), :]
        mixed = jnp.where(column[p] == 0, mixed[:, :128], mixed[:, 128:]).astype(F32)
        outv[p - 1, rows(r), :] = (mixed + total).astype(BF16)
        columns = pl.ds(pl.multiple_of(column[p] * 128, 128), 128)
        store = local(("out", p, r), outv.at[p - 1, rows(r)], out.at[rows(r), columns])
        store.start()
        stores.append(store)

    def norm(src, gain, r):
        def body(i, carry):
            at = pl.ds(pl.multiple_of(r * CH + i * 64, 64), 64)
            square = jnp.zeros((64, DV), F32)
            for b in range(8):
                v = src[b, at, :].astype(F32)
                square = square + v * v
            mean = jnp.sum(square, axis=-1, keepdims=True) * (1.0 / D)
            scale = lax.rsqrt(mean + EPS)
            for b in range(8):
                v = src[b, at, :].astype(F32)
                g = gain[pl.ds(b * DV, DV)].reshape(1, DV).astype(F32)
                nrm[at, b * DV : (b + 1) * DV] = (v * scale * g).astype(BF16)
            return carry

        lax.fori_loop(0, CH // 64, body, 0, unroll=2)

    def decays():
        rt = rate[0]
        i = lax.broadcasted_iota(jnp.int32, (CH, CH), 0)
        j = lax.broadcasted_iota(jnp.int32, (CH, CH), 1)
        near = (i - j).astype(F32)
        for d in range(NCH):
            dist = near + float(d * CH)
            value = jnp.exp(-rt * jnp.maximum(dist, 0.0)) * DK ** (-0.5)
            dec[d] = jnp.where(dist >= 0.0, value, 0.0)

    def dot(a, b):
        return jnp.dot(a, b, preferred_element_type=F32)

    def mixa(r):
        a = nrm[rows(r), :]
        qkv = dot(a, wq[:, :, :, 0 : 2 * DK + DV].reshape(D, 2 * DK + DV))
        q = qkv[:, :DK].astype(BF16)
        kbuf[rows(r), :] = qkv[:, DK : 2 * DK].astype(BF16)
        vbuf[rows(r), :] = qkv[:, 2 * DK :].astype(BF16)
        gate = dot(a, wq[:, :, :, 2 * DK + DV :].reshape(D, DV))
        kept = jnp.zeros((CH, DV), F32)
        for b in range(r + 1):
            score = lax.dot_general(
                q, kbuf[rows(b), :], (((1,), (1,)), ((), ())), preferred_element_type=F32
            )
            score = (score * dec[r - b]).astype(BF16)
            kept = kept + dot(score, vbuf[rows(b), :])
        mean = jnp.mean(kept * kept, axis=-1, keepdims=True)
        kept = kept * lax.rsqrt(mean + EPS)
        hid[rows(r), :] = (gate / (1.0 + jnp.exp(-gate)) * kept).astype(BF16)

    def mix(r):
        own, snd = sums[0][:2]
        for b in range(4):
            for dst, cc in ((snd, other), (own, c)):
                right = jnp.concatenate([wo[b, 2 * cc], wo[b, 2 * cc + 1]], axis=1)
                dst[b, rows(r), :] = dot(hid[rows(r), :], right).astype(BF16)

    def up(r):
        a = nrm[rows(r), :]
        for b in range(4):
            upward = dot(a, wu[:, :, :, b * 256 : (b + 1) * 256].reshape(D, 256))
            upward = jnp.maximum(upward, 0.0)
            act[rows(r), b * 256 : (b + 1) * 256] = (upward * upward).astype(BF16)

    def down(p, r):
        own, snd = sums[p][:2]
        for b in (0, 2):
            for dst, cc in ((snd, other), (own, c)):
                at = 2 * cc + column[p]
                right = jnp.concatenate([wd[b, at], wd[b + 1, at]], axis=1)
                value = dot(act[rows(r), :], right).astype(BF16)
                dst[b, rows(r), :] = value[:, :128]
                dst[b + 1, rows(r), :] = value[:, 128:]

    def load(names):
        for name in names:
            loads[name].wait()

    feats = {"t": (xg, gmix), "m": (mg, gmlp)}
    kinds = {"w3": w3, "w4": w4, "w5": w5}
    plain = {
        "load": load, "w1": w1, "w2": w2, "s0": s0, "s1": s1, "s2": s2, "s3": s3,
        "mixa": mixa, "mix": mix, "up": up, "down": down, "decays": decays,
    }
    gathers = {"g1": g1, "g2": g2, "g3": g3, "g4": g4}
    for name, *args in ORDER:
        if name == "norm":
            norm(*feats[args[0]], args[1])
        elif name in gathers:
            gathers[name](args[0], feats[args[0]][0], args[1])
        elif name in plain:
            plain[name](*args)
        else:
            kinds[name[:2]](name[2], *args)
    for copy in sent:
        copy.wait_send()
    for store in stores:
        store.wait()


def local(
    tokens, gain_mix, query_weight, key_weight, value_weight, gate_weight,
    decay_rate, out_weight, gain_mlp, up_weight, down_weight,
):
    hbm = pl.BlockSpec(memory_space=pl.ANY)
    vmem = pl.BlockSpec(memory_space=pltpu.VMEM)
    smem = pl.BlockSpec(memory_space=pltpu.SMEM)

    def summing(width):
        whole = [pltpu.VMEM((4, SEQ, width), BF16)] * 3
        moved = [pltpu.VMEM((NCH, n, width), BF16) for n in (HC, HC, CH, CH)]
        return whole + moved + moved

    return pl.pallas_call(
        kernel,
        out_shape=jax.ShapeDtypeStruct((SEQ, DV), BF16),
        in_specs=[hbm, vmem, hbm, hbm, hbm, hbm, smem, hbm, vmem, hbm, hbm],
        out_specs=hbm,
        scratch_shapes=[
            pltpu.VMEM((8, SEQ, DV), BF16),
            pltpu.VMEM((8, SEQ, DV), BF16),
            pltpu.VMEM((SEQ, D), BF16),
            pltpu.VMEM((4, 4, 128, 768), BF16),
            pltpu.VMEM((4, 4, 256, 128), BF16),
            pltpu.VMEM((4, 4, 128, 1024), BF16),
            pltpu.VMEM((4, 4, 1024, 128), BF16),
            pltpu.VMEM((SEQ, DK), BF16),
            pltpu.VMEM((SEQ, DV), BF16),
            pltpu.VMEM((NCH, CH, CH), F32),
            pltpu.VMEM((SEQ, DV), BF16),
            pltpu.VMEM((SEQ, 1024), BF16),
            pltpu.VMEM((2, SEQ, 128), BF16),
            pltpu.SemaphoreType.DMA((N_REMOTE,)),
            pltpu.SemaphoreType.DMA((N_REMOTE,)),
            pltpu.SemaphoreType.DMA((N_LOCAL,)),
            *summing(DV), *summing(128), *summing(128),
        ],
        compiler_params=pltpu.CompilerParams(
            collective_id=0, has_side_effects=True, vmem_limit_bytes=62 * 1024 * 1024
        ),
    )(
        tokens, gain_mix, query_weight, key_weight, value_weight, gate_weight,
        decay_rate, out_weight, gain_mlp, up_weight, down_weight,
    )


def solution(mesh):
    finer = Mesh(
        mesh.devices.reshape(mesh.shape["rep"], 4, 4, 4, 2), ("rep", "zl", "x", "y", "c")
    )
    placed = (
        P(("rep", "zl", "x"), TP), P(), P(FS, TP), P(FS, TP), P(FS, TP), P(FS, TP),
        P(TP), P(TP, FS), P(), P(FS, TP), P(TP, FS),
    )
    return jax.shard_map(
        local, mesh=finer, in_specs=placed, out_specs=P(("rep", "zl", "x"), TP), check_vma=False
    )
```

```python
import functools

import jax
import jax.numpy as jnp
from jax import lax
from jax.experimental import pallas as pl
from jax.experimental.pallas import tpu as pltpu
from jax.sharding import Mesh
from jax.sharding import PartitionSpec as P

DK = 128
DV = 256
SEQ = 768
D = 2048
CH = 256
NCH = SEQ // CH
HC = CH // 2
EPS = 1e-06
F32 = jnp.float32
BF16 = jnp.bfloat16
TP = ("y", "c")
FS = ("zl", "x")
ORDER = [
    ('load', 'ud'), ('load', 'qkvg'), ('load', 't'), ('w1', 'q', 'B'), ('w1', 'q', 'A'), ('g1', 't', 1),
    ('load', 'o'), ('w1', 'o', 'B'), ('w3o', 'o', 'A'), ('g1', 't', 2), ('w1', 'o', 'A'), ('w3o', 'q', 'B'),
    ('w3o', 'q', 'A'), ('w1', 'u', 'A'), ('g1', 't', 0), ('w3o', 'o', 'B'), ('w1', 'u', 'B'),
    ('w2', 'q', 'A'), ('w2', 'o', 'B'), ('w2', 'o', 'A'), ('w2', 'q', 'B'), ('w3n', 'q', 'A'),
    ('w3n', 'o', 'A'), ('w3n', 'q', 'B'), ('g2', 't', 1), ('w3f', 'o', 'A'), ('w3f', 'q', 'A'),
    ('g3', 't', 1), ('w4o', 'q', 'A'), ('w4o', 'o', 'B'), ('w4o', 'o', 'A'), ('w3f', 'q', 'B'),
    ('w3f', 'o', 'B'), ('w3n', 'o', 'B'), ('decays',), ('g2', 't', 0), ('g4', 't', 1), ('w4n', 'q', 'A'),
    ('w4o', 'q', 'B'), ('g2', 't', 2), ('w4n', 'q', 'B'), ('norm', 't', 1), ('w4f', 'q', 'B'),
    ('w4f', 'q', 'A'), ('w4n', 'o', 'B'), ('w5o', 'o', 'A'), ('w4n', 'o', 'A'), ('g3', 't', 0),
    ('w4f', 'o', 'A'), ('g3', 't', 2), ('w4f', 'o', 'B'), ('g4', 't', 2), ('w3o', 'u', 'B'), ('w2', 'u', 'B'),
    ('g4', 't', 0), ('w5o', 'q', 'A'), ('w1', 'd', 'B'), ('w5n', 'q', 'B'), ('norm', 't', 2),
    ('norm', 't', 0), ('w5f', 'q', 'B'), ('w2', 'u', 'A'), ('w5f', 'q', 'A'), ('w5n', 'q', 'A'),
    ('w5o', 'o', 'B'), ('w3o', 'u', 'A'), ('w5o', 'q', 'B'), ('w1', 'd', 'A'), ('mixa', 0), ('w5n', 'o', 'A'),
    ('w5n', 'o', 'B'), ('w5f', 'o', 'A'), ('w5f', 'o', 'B'), ('mix', 0), ('s0', 0, 0), ('mixa', 1),
    ('w3n', 'u', 'A'), ('mix', 1), ('s0', 0, 1), ('s1', 0, 0), ('w3f', 'u', 'B'), ('mixa', 2), ('mix', 2),
    ('s0', 0, 2), ('s1', 0, 1), ('w3n', 'u', 'B'), ('s1', 0, 2), ('w2', 'd', 'A'), ('s2', 0, 0),
    ('w2', 'd', 'B'), ('s2', 0, 1), ('w4o', 'u', 'B'), ('w3f', 'u', 'A'), ('s2', 0, 2), ('s3', 0, 0),
    ('g1', 'm', 0), ('w4n', 'u', 'A'), ('w3n', 'd', 'A'), ('w3n', 'd', 'B'), ('w4f', 'u', 'B'),
    ('w4f', 'u', 'A'), ('w5o', 'u', 'B'), ('w4o', 'u', 'A'), ('s3', 0, 2), ('g1', 'm', 2), ('w4n', 'u', 'B'),
    ('w3o', 'd', 'A'), ('s3', 0, 1), ('g2', 'm', 0), ('g1', 'm', 1), ('w3f', 'd', 'B'), ('w3o', 'd', 'B'),
    ('g2', 'm', 2), ('w4n', 'd', 'A'), ('w5n', 'u', 'A'), ('w5f', 'u', 'A'), ('w3f', 'd', 'A'),
    ('g3', 'm', 0), ('g2', 'm', 1), ('w5n', 'u', 'B'), ('g4', 'm', 0), ('norm', 'm', 0), ('w4n', 'd', 'B'),
    ('w5f', 'u', 'B'), ('w5o', 'u', 'A'), ('g3', 'm', 2), ('up', 0), ('w4f', 'd', 'B'), ('w4o', 'd', 'A'),
    ('g4', 'm', 2), ('norm', 'm', 2), ('up', 2), ('g3', 'm', 1), ('w5n', 'd', 'A'), ('w4o', 'd', 'B'),
    ('down', 1, 2), ('s0', 1, 2), ('down', 1, 0), ('s0', 1, 0), ('g4', 'm', 1), ('s1', 1, 2),
    ('norm', 'm', 1), ('w4f', 'd', 'A'), ('s1', 1, 0), ('up', 1), ('down', 1, 1), ('w5f', 'd', 'B'),
    ('s0', 1, 1), ('s2', 1, 2), ('s1', 1, 1), ('w5o', 'd', 'A'), ('w5n', 'd', 'B'), ('w5o', 'd', 'B'),
    ('s2', 1, 0), ('w5f', 'd', 'A'), ('down', 2, 2), ('s0', 2, 2), ('down', 2, 1), ('s0', 2, 1), ('s1', 2, 2),
    ('down', 2, 0), ('s1', 2, 1), ('s3', 1, 2), ('s0', 2, 0), ('s2', 1, 1), ('s1', 2, 0), ('s2', 2, 2),
    ('s3', 1, 0), ('s2', 2, 1), ('s3', 1, 1), ('s2', 2, 0), ('s3', 2, 1), ('s3', 2, 2), ('s3', 2, 0),
]
MESH_ID = pl.DeviceIdType.MESH
N_SENDS = 20
N_ARRIVALS = 97
N_LOCAL = 6


def kernel(
    tok, gmix, qw, kw, vw, gw, rate, ow, gmlp, uw, dw,
    out,
    xg, mg, nrm, wq, wo, wu, wd, kbuf, vbuf, dec, hid, act, outv,
    send_sem, recv_sem, local_sem, *summing,
):
    sums = [summing[11 * p : 11 * p + 11] for p in range(3)]
    rep, zl = lax.axis_index("rep"), lax.axis_index("zl")
    x, y, c = lax.axis_index("x"), lax.axis_index("y"), lax.axis_index("c")

    def mod4(v):
        return lax.rem(v + 4, 4)

    def z_id(step):
        z = lax.rem(rep * 4 + zl + step + 8, 8)
        return {"rep": z // 4, "zl": lax.rem(z, 4)}

    xp, xm, x2 = mod4(x + 1), mod4(x - 1), mod4(x + 2)
    zp, zm, z2 = mod4(zl + 1), mod4(zl - 1), mod4(zl + 2)
    yp, ym, y2 = mod4(y + 1), mod4(y - 1), mod4(y + 2)
    to_xp, to_xm = {"x": xp}, {"x": xm}
    to_zp, to_zm = z_id(1), z_id(-1)
    to_yp, to_ym = {"y": yp}, {"y": ym}
    to_pair = {"c": 1 - c}

    sends, arrivals = {}, {}

    def remote(out_group, in_group, src, dst, dev):
        i = sends.setdefault(out_group, len(sends))
        j = arrivals.setdefault(in_group, len(arrivals))
        return pltpu.make_async_remote_copy(
            src_ref=src,
            dst_ref=dst,
            send_sem=send_sem.at[i],
            recv_sem=recv_sem.at[j],
            device_id=dev,
            device_id_type=MESH_ID,
        )

    def send(out_group, in_group, src, dst, dev):
        remote(out_group, in_group, src, dst, dev).start()

    def arrived(in_group, whole, dev):
        remote(next(iter(sends)), in_group, whole, whole, dev).wait_recv()

    me = y * 2 + c
    wq_own = wq.at[zl, x]
    loads = [
        (0, tok, xg.at[me]),
        (1, qw, wq_own.at[:, pl.ds(0, DK)]),
        (1, kw, wq_own.at[:, pl.ds(DK, DK)]),
        (1, vw, wq_own.at[:, pl.ds(2 * DK, DV)]),
        (1, gw, wq_own.at[:, pl.ds(2 * DK + DV, DV)]),
        (2, ow, wo.at[zl, x]),
        (3, uw, wu.at[zl, x]),
        (4, dw, wd.at[zl, x]),
    ]
    for i, src, dst in loads:
        pltpu.make_async_copy(src, dst, local_sem.at[i]).start()

    barrier = pltpu.get_barrier_semaphore()
    for dev in (to_xp, to_xm, to_zp, to_zm, to_yp, to_ym, to_pair):
        pl.semaphore_signal(barrier, inc=1, device_id=dev, device_id_type=MESH_ID)
    pl.semaphore_wait(barrier, 7)

    weights = {"q": (wq, 128), "o": (wo, 256), "u": (wu, 128), "d": (wd, 1024)}

    def slab(w, half, first, second, quarter=None):
        buf, n = weights[w]
        start, size = (0 if half == "A" else n // 2), n // 2
        if quarter is not None:
            size //= 2
            start += quarter * size
        zi, xi = (second, first) if half == "A" else (first, second)
        return buf.at[zi, xi, pl.ds(start, size)]

    ring_x = (x, xp, xm, x2, to_xp, to_xm)
    ring_z = (zl, zp, zm, z2, to_zp, to_zm)

    def rings(half):
        return (ring_x, ring_z) if half == "A" else (ring_z, ring_x)

    def shards(w, n):
        buf = weights[w][0]
        return buf.at[0, pl.ds(0, n)]

    def half_shard(w):
        buf, n = weights[w]
        return buf.at[0, 0, pl.ds(0, n // 2)]

    def w1(w, half):
        (at, _, _, _, plus, minus), (here, *_) = rings(half)
        s = slab(w, half, at, here)
        send((w, "first"), (w, half, 1), s, s, plus)
        send((w, "first"), (w, half, 1), s, s, minus)

    def w2(w, half):
        (_, up, dn, _, plus, minus), (here, *_) = rings(half)
        arrived((w, half, 1), shards(w, 1), plus)
        s = slab(w, half, dn, here, 0)
        send((w, "first"), (w, half, 2), s, s, plus)
        s = slab(w, half, up, here, 1)
        send((w, "first"), (w, half, 2), s, s, minus)

    def slabs_of(kind, ring):
        at, up, dn, far, _, _ = ring
        return {"o": [at], "n": [up, dn], "f": [far]}[kind]

    def w3(kind, w, half):
        first, (here, _, _, _, plus, minus) = rings(half)
        if kind == "f":
            arrived((w, half, 2), half_shard(w), first[4])
        for i in slabs_of(kind, first):
            s = slab(w, half, i, here)
            send((w, "third"), (w, half, 3, kind), s, s, plus)
            send((w, "third"), (w, half, 3, kind), s, s, minus)

    def last_group(kind, w, half):
        return (w, half, 4, kind if w == "d" else "all")

    def w4(kind, w, half):
        first, (_, up, dn, _, plus, minus) = rings(half)
        slabs = slabs_of(kind, first)
        arrived((w, half, 3, kind), shards(w, len(slabs)), plus)
        for i in slabs:
            s = slab(w, half, i, dn, 0)
            send((w, "fourth"), last_group(kind, w, half), s, s, plus)
            s = slab(w, half, i, up, 1)
            send((w, "fourth"), last_group(kind, w, half), s, s, minus)

    seen = {}

    def w5(kind, w, half):
        plus = rings(half)[1][4]
        seen[w, half] = seen.get((w, half), 0) + 1
        if w == "d":
            ref = shards(w, 1) if kind == "n" else half_shard(w)
            arrived(last_group(kind, w, half), ref, plus)
        elif seen[w, half] == 3:
            arrived(last_group(kind, w, half), shards(w, 2), plus)

    def rows(r):
        return pl.ds(r * CH, CH)

    blk = lambda yy, cc: yy * 2 + cc
    other = 1 - c

    def part(buf, b, r, half=None):
        if half is None:
            return buf.at[b, pl.ds(r * CH, CH)]
        return buf.at[b, pl.ds(r * CH + half * HC, HC)]

    def g1(tag, buf, r):
        s = part(buf, blk(y, c), r)
        send(tag, (tag, r, 1), s, s, to_yp)
        send(tag, (tag, r, 1), s, s, to_ym)
        send(tag, (tag, r, 3), s, s, to_pair)

    def g2(tag, buf, r):
        arrived((tag, r, 1), buf.at[pl.ds(0, 2), rows(r)], to_yp)
        s = part(buf, blk(ym, c), r, 0)
        send(tag, (tag, r, 2), s, s, to_yp)
        s = part(buf, blk(yp, c), r, 1)
        send(tag, (tag, r, 2), s, s, to_ym)
        s = part(buf, blk(ym, c), r)
        send(tag, (tag, r, 3), s, s, to_pair)
        s = part(buf, blk(yp, c), r)
        send(tag, (tag, r, 3), s, s, to_pair)

    def g3(tag, buf, r):
        s = part(buf, blk(y2, c), r)
        arrived((tag, r, 2), s, to_yp)
        send(tag, (tag, r, 3), s, s, to_pair)

    def g4(tag, buf, r):
        arrived((tag, r, 3), buf.at[pl.ds(0, 4), rows(r)], to_pair)

    def s0(p, r):
        own, snd, prc = sums[p][:3]
        send(("pair", p), (p, r, 0), snd.at[:, rows(r)], prc.at[:, rows(r)], to_pair)

    def pair_sum(p, r, b, lo, n):
        own, snd, prc = sums[p][:3]
        at = pl.ds(r * CH + lo, n)
        return own[b, at, :].astype(F32) + prc[b, at, :].astype(F32)

    def s1(p, r):
        _, _, prc, s_a, s_b, _, _, r_a, r_b, _, _ = sums[p]
        arrived((p, r, 0), prc.at[:, rows(r)], to_pair)
        s_a[r] = pair_sum(p, r, y2, 0, HC).astype(BF16)
        send(("ring", p), (p, r, 1), s_a.at[r], r_a.at[r], to_yp)
        s_b[r] = pair_sum(p, r, y2, HC, HC).astype(BF16)
        send(("ring", p), (p, r, 1), s_b.at[r], r_b.at[r], to_ym)

    def s2(p, r):
        own, _, _, _, _, s_p, s_m, r_a, r_b, r_p, r_m = sums[p]
        s_p[r, pl.ds(HC, HC)] = pair_sum(p, r, yp, HC, HC).astype(BF16)
        s_m[r, pl.ds(0, HC)] = pair_sum(p, r, ym, 0, HC).astype(BF16)
        arrived((p, r, 1), own.at[0, rows(r)], to_yp)
        s_p[r, pl.ds(0, HC)] = (pair_sum(p, r, yp, 0, HC) + r_a[r].astype(F32)).astype(BF16)
        send(("ring", p), (p, r, 2), s_p.at[r], r_p.at[r], to_yp)
        s_m[r, pl.ds(HC, HC)] = (pair_sum(p, r, ym, HC, HC) + r_b[r].astype(F32)).astype(BF16)
        send(("ring", p), (p, r, 2), s_m.at[r], r_m.at[r], to_ym)

    odd = lax.rem(x, 2)
    column = {1: 1 - odd, 2: odd}

    def s3(p, r):
        own, r_p, r_m = sums[p][0], sums[p][9], sums[p][10]
        total = pair_sum(p, r, y, 0, CH)
        arrived((p, r, 2), own.at[pl.ds(0, 2), rows(r)], to_yp)
        total = total + (r_p[r].astype(F32) + r_m[r].astype(F32))
        if p == 0:
            mg[me, rows(r), :] = (xg[me, rows(r), :].astype(F32) + total).astype(BF16)
            return
        mixed = mg[me, rows(r), :]
        mixed = jnp.where(column[p] == 0, mixed[:, :128], mixed[:, 128:]).astype(F32)
        outv[p - 1, rows(r), :] = (mixed + total).astype(BF16)
        columns = pl.ds(pl.multiple_of(column[p] * 128, 128), 128)
        pltpu.make_async_copy(
            outv.at[p - 1, rows(r)], out.at[rows(r), columns], local_sem.at[5]
        ).start()

    def norm(src, gain, r):
        def body(i, carry):
            at = pl.ds(pl.multiple_of(r * CH + i * 64, 64), 64)
            square = jnp.zeros((64, DV), F32)
            for b in range(8):
                v = src[b, at, :].astype(F32)
                square = square + v * v
            mean = jnp.sum(square, axis=-1, keepdims=True) * (1.0 / D)
            scale = lax.rsqrt(mean + EPS)
            for b in range(8):
                v = src[b, at, :].astype(F32)
                g = gain[pl.ds(b * DV, DV)].reshape(1, DV).astype(F32)
                nrm[at, b * DV : (b + 1) * DV] = (v * scale * g).astype(BF16)
            return carry

        lax.fori_loop(0, CH // 64, body, 0, unroll=2)

    def decays():
        rt = rate[0]
        i = lax.broadcasted_iota(jnp.int32, (CH, CH), 0)
        j = lax.broadcasted_iota(jnp.int32, (CH, CH), 1)
        near = (i - j).astype(F32)
        for d in range(NCH):
            dist = near + float(d * CH)
            value = jnp.exp(-rt * jnp.maximum(dist, 0.0)) * DK ** (-0.5)
            dec[d] = jnp.where(dist >= 0.0, value, 0.0)

    def dot(a, b):
        return jnp.dot(a, b, preferred_element_type=F32)

    def mixa(r):
        a = nrm[rows(r), :]
        qkv = dot(a, wq[:, :, :, 0 : 2 * DK + DV].reshape(D, 2 * DK + DV))
        q = qkv[:, :DK].astype(BF16)
        kbuf[rows(r), :] = qkv[:, DK : 2 * DK].astype(BF16)
        vbuf[rows(r), :] = qkv[:, 2 * DK :].astype(BF16)
        gate = dot(a, wq[:, :, :, 2 * DK + DV :].reshape(D, DV))
        kept = jnp.zeros((CH, DV), F32)
        for b in range(r + 1):
            score = lax.dot_general(
                q, kbuf[rows(b), :], (((1,), (1,)), ((), ())), preferred_element_type=F32
            )
            score = (score * dec[r - b]).astype(BF16)
            kept = kept + dot(score, vbuf[rows(b), :])
        mean = jnp.mean(kept * kept, axis=-1, keepdims=True)
        kept = kept * lax.rsqrt(mean + EPS)
        hid[rows(r), :] = (gate / (1.0 + jnp.exp(-gate)) * kept).astype(BF16)

    def mix(r):
        own, snd = sums[0][:2]
        for b in range(4):
            for dst, cc in ((snd, other), (own, c)):
                right = jnp.concatenate([wo[b, 2 * cc], wo[b, 2 * cc + 1]], axis=1)
                dst[b, rows(r), :] = dot(hid[rows(r), :], right).astype(BF16)

    def up(r):
        a = nrm[rows(r), :]
        for b in range(4):
            upward = dot(a, wu[:, :, :, b * 256 : (b + 1) * 256].reshape(D, 256))
            upward = jnp.maximum(upward, 0.0)
            act[rows(r), b * 256 : (b + 1) * 256] = (upward * upward).astype(BF16)

    def down(p, r):
        own, snd = sums[p][:2]
        for b in (0, 2):
            for dst, cc in ((snd, other), (own, c)):
                at = 2 * cc + column[p]
                right = jnp.concatenate([wd[b, at], wd[b + 1, at]], axis=1)
                value = dot(act[rows(r), :], right).astype(BF16)
                dst[b, rows(r), :] = value[:, :128]
                dst[b + 1, rows(r), :] = value[:, 128:]

    def load(names):
        for i, ref in enumerate((xg.at[me], wq_own, wo.at[zl, x], wu.at[zl, x], wd.at[zl, x])):
            if "tqoud"[i] in names:
                pltpu.make_async_copy(ref, ref, local_sem.at[i]).wait()

    feats = {"t": (xg, gmix), "m": (mg, gmlp)}
    kinds = {"w3": w3, "w4": w4, "w5": w5}
    plain = {
        "load": load, "w1": w1, "w2": w2, "s0": s0, "s1": s1, "s2": s2, "s3": s3,
        "mixa": mixa, "mix": mix, "up": up, "down": down, "decays": decays,
    }
    gathers = {"g1": g1, "g2": g2, "g3": g3, "g4": g4}
    for name, *args in ORDER:
        if name == "norm":
            norm(*feats[args[0]], args[1])
        elif name in gathers:
            gathers[name](args[0], feats[args[0]][0], args[1])
        elif name in plain:
            plain[name](*args)
        else:
            kinds[name[:2]](name[2], *args)
    def left(out_group, whole):
        remote(out_group, next(iter(arrivals)), whole, whole, to_pair).wait_send()

    for w, (buf, _) in weights.items():
        left((w, "first"), shards(w, 3))
        left((w, "third"), buf.at[pl.ds(0, 2)])
        left((w, "fourth"), shards(w, 4))
    for tag, (buf, _) in feats.items():
        left(tag, buf.at[pl.ds(0, 7)])
    for p in range(3):
        own = sums[p][0]
        left(("pair", p), own)
        left(("ring", p), own.at[pl.ds(0, 3)])
    pltpu.make_async_copy(outv, outv, local_sem.at[5]).wait()


def local(
    tokens, gain_mix, query_weight, key_weight, value_weight, gate_weight,
    decay_rate, out_weight, gain_mlp, up_weight, down_weight,
):
    hbm = pl.BlockSpec(memory_space=pltpu.HBM)
    vmem = pl.BlockSpec(memory_space=pltpu.VMEM)
    smem = pl.BlockSpec(memory_space=pltpu.SMEM)

    def summing(width):
        whole = [pltpu.VMEM((4, SEQ, width), BF16)] * 3
        moved = [pltpu.VMEM((NCH, n, width), BF16) for n in (HC, HC, CH, CH)]
        return whole + moved + moved

    return pl.pallas_call(
        kernel,
        out_shape=jax.ShapeDtypeStruct((SEQ, DV), BF16),
        in_specs=[hbm, vmem, hbm, hbm, hbm, hbm, smem, hbm, vmem, hbm, hbm],
        out_specs=hbm,
        scratch_shapes=[
            pltpu.VMEM((8, SEQ, DV), BF16),
            pltpu.VMEM((8, SEQ, DV), BF16),
            pltpu.VMEM((SEQ, D), BF16),
            pltpu.VMEM((4, 4, 128, 768), BF16),
            pltpu.VMEM((4, 4, 256, 128), BF16),
            pltpu.VMEM((4, 4, 128, 1024), BF16),
            pltpu.VMEM((4, 4, 1024, 128), BF16),
            pltpu.VMEM((SEQ, DK), BF16),
            pltpu.VMEM((SEQ, DV), BF16),
            pltpu.VMEM((NCH, CH, CH), F32),
            pltpu.VMEM((SEQ, DV), BF16),
            pltpu.VMEM((SEQ, 1024), BF16),
            pltpu.VMEM((2, SEQ, 128), BF16),
            pltpu.SemaphoreType.DMA((N_SENDS,)),
            pltpu.SemaphoreType.DMA((N_ARRIVALS,)),
            pltpu.SemaphoreType.DMA((N_LOCAL,)),
            *summing(DV), *summing(128), *summing(128),
        ],
        compiler_params=pltpu.CompilerParams(
            collective_id=0, has_side_effects=True, vmem_limit_bytes=62 * 1024 * 1024
        ),
    )(
        tokens, gain_mix, query_weight, key_weight, value_weight, gate_weight,
        decay_rate, out_weight, gain_mlp, up_weight, down_weight,
    )


def solution(mesh):
    finer = Mesh(
        mesh.devices.reshape(mesh.shape["rep"], 4, 4, 4, 2), ("rep", "zl", "x", "y", "c")
    )
    placed = (
        P(("rep", "zl", "x"), TP), P(), P(FS, TP), P(FS, TP), P(FS, TP), P(FS, TP),
        P(TP), P(TP, FS), P(), P(FS, TP), P(TP, FS),
    )
    return jax.shard_map(
        local, mesh=finer, in_specs=placed, out_specs=P(("rep", "zl", "x"), TP), check_vma=False
    )
```

```python
import functools

import jax
import jax.numpy as jnp
from jax import lax
from jax.experimental import pallas as pl
from jax.experimental.pallas import tpu as pltpu
from jax.sharding import Mesh
from jax.sharding import PartitionSpec as P

DK = 128
DV = 256
SEQ = 768
D = 2048
CH = 256
NCH = SEQ // CH
HC = CH // 2
EPS = 1e-06
F32 = jnp.float32
BF16 = jnp.bfloat16
TP = ("y", "c")
FS = ("zl", "x")
ORDER = [
    ('load', 'ud'), ('load', 'qkvg'), ('load', 't'), ('w1', 'q', 'B'), ('w1', 'q', 'A'), ('g1', 't', 1),
    ('load', 'o'), ('w1', 'o', 'B'), ('w3o', 'o', 'A'), ('g1', 't', 2), ('w1', 'o', 'A'), ('w3o', 'q', 'B'),
    ('w3o', 'q', 'A'), ('w1', 'u', 'A'), ('g1', 't', 0), ('w3o', 'o', 'B'), ('w1', 'u', 'B'),
    ('w2', 'q', 'A'), ('w2', 'o', 'B'), ('w2', 'o', 'A'), ('w2', 'q', 'B'), ('w3n', 'q', 'A'),
    ('w3n', 'o', 'A'), ('w3n', 'q', 'B'), ('g2', 't', 1), ('w3f', 'o', 'A'), ('w3f', 'q', 'A'),
    ('g3', 't', 1), ('w4o', 'q', 'A'), ('w4o', 'o', 'B'), ('w4o', 'o', 'A'), ('w3f', 'q', 'B'),
    ('w3f', 'o', 'B'), ('w3n', 'o', 'B'), ('g2', 't', 0), ('g4', 't', 1), ('w4n', 'q', 'A'),
    ('w4o', 'q', 'B'), ('g2', 't', 2), ('w4n', 'q', 'B'), ('load', 'a'), ('norm', 't', 1), ('w4f', 'q', 'B'),
    ('w4f', 'q', 'A'), ('w4n', 'o', 'B'), ('w5o', 'o', 'A'), ('w4n', 'o', 'A'), ('g3', 't', 0),
    ('w4f', 'o', 'A'), ('g3', 't', 2), ('w4f', 'o', 'B'), ('g4', 't', 2), ('w3o', 'u', 'B'), ('w2', 'u', 'B'),
    ('g4', 't', 0), ('w5o', 'q', 'A'), ('w1', 'd', 'B'), ('w5n', 'q', 'B'), ('norm', 't', 2),
    ('norm', 't', 0), ('w5f', 'q', 'B'), ('w2', 'u', 'A'), ('w5f', 'q', 'A'), ('w5n', 'q', 'A'),
    ('w5o', 'o', 'B'), ('w3o', 'u', 'A'), ('w5o', 'q', 'B'), ('w1', 'd', 'A'), ('mixa', 0), ('w5n', 'o', 'A'),
    ('w5n', 'o', 'B'), ('w5f', 'o', 'A'), ('w5f', 'o', 'B'), ('mix', 0), ('s0', 0, 0), ('mixa', 1),
    ('w3n', 'u', 'A'), ('mix', 1), ('s0', 0, 1), ('s1', 0, 0), ('w3f', 'u', 'B'), ('mixa', 2), ('mix', 2),
    ('s0', 0, 2), ('s1', 0, 1), ('w3n', 'u', 'B'), ('s1', 0, 2), ('w2', 'd', 'A'), ('s2', 0, 0),
    ('w2', 'd', 'B'), ('s2', 0, 1), ('w4o', 'u', 'B'), ('w3f', 'u', 'A'), ('s2', 0, 2), ('s3', 0, 0),
    ('g1', 'm', 0), ('w4n', 'u', 'A'), ('w3n', 'd', 'A'), ('w3n', 'd', 'B'), ('w4f', 'u', 'B'),
    ('w4f', 'u', 'A'), ('w5o', 'u', 'B'), ('w4o', 'u', 'A'), ('s3', 0, 2), ('g1', 'm', 2), ('w4n', 'u', 'B'),
    ('w3o', 'd', 'A'), ('s3', 0, 1), ('g2', 'm', 0), ('g1', 'm', 1), ('w3f', 'd', 'B'), ('w3o', 'd', 'B'),
    ('g2', 'm', 2), ('w4n', 'd', 'A'), ('w5n', 'u', 'A'), ('w5f', 'u', 'A'), ('w3f', 'd', 'A'),
    ('g3', 'm', 0), ('g2', 'm', 1), ('w5n', 'u', 'B'), ('g4', 'm', 0), ('load', 'b'), ('norm', 'm', 0),
    ('w4n', 'd', 'B'), ('w5f', 'u', 'B'), ('w5o', 'u', 'A'), ('g3', 'm', 2), ('up', 0), ('w4f', 'd', 'B'),
    ('w4o', 'd', 'A'), ('g4', 'm', 2), ('norm', 'm', 2), ('up', 2), ('g3', 'm', 1), ('w5n', 'd', 'A'),
    ('w4o', 'd', 'B'), ('down', 1, 2), ('s0', 1, 2), ('down', 1, 0), ('s0', 1, 0), ('g4', 'm', 1),
    ('s1', 1, 2), ('norm', 'm', 1), ('w4f', 'd', 'A'), ('s1', 1, 0), ('up', 1), ('down', 1, 1),
    ('w5f', 'd', 'B'), ('s0', 1, 1), ('s2', 1, 2), ('s1', 1, 1), ('w5o', 'd', 'A'), ('w5n', 'd', 'B'),
    ('w5o', 'd', 'B'), ('s2', 1, 0), ('w5f', 'd', 'A'), ('down', 2, 2), ('s0', 2, 2), ('down', 2, 1),
    ('s0', 2, 1), ('s1', 2, 2), ('down', 2, 0), ('s1', 2, 1), ('s3', 1, 2), ('s0', 2, 0), ('s2', 1, 1),
    ('s1', 2, 0), ('s2', 2, 2), ('s3', 1, 0), ('s2', 2, 1), ('s3', 1, 1), ('s2', 2, 0), ('s3', 2, 1),
    ('s3', 2, 2), ('s3', 2, 0),
]
MESH_ID = pl.DeviceIdType.MESH
N_SENDS = 20
N_ARRIVALS = 97
N_LOCAL = 7


def kernel(
    tok, gain_mix, qw, kw, vw, gw, rate, ow, gain_mlp, uw, dw,
    out,
    gmix, gmlp, xg, mg, nrm, wq, wo, wu, wd, kbuf, vbuf, dec, hid, act,
    send_sem, recv_sem, local_sem, *summing,
):
    sums = [summing[11 * p : 11 * p + 11] for p in range(3)]
    rep, zl = lax.axis_index("rep"), lax.axis_index("zl")
    x, y, c = lax.axis_index("x"), lax.axis_index("y"), lax.axis_index("c")

    def mod4(v):
        return lax.rem(v + 4, 4)

    def z_id(step):
        z = lax.rem(rep * 4 + zl + step + 8, 8)
        return {"rep": z // 4, "zl": lax.rem(z, 4)}

    xp, xm, x2 = mod4(x + 1), mod4(x - 1), mod4(x + 2)
    zp, zm, z2 = mod4(zl + 1), mod4(zl - 1), mod4(zl + 2)
    yp, ym, y2 = mod4(y + 1), mod4(y - 1), mod4(y + 2)
    to_xp, to_xm = {"x": xp}, {"x": xm}
    to_zp, to_zm = z_id(1), z_id(-1)
    to_yp, to_ym = {"y": yp}, {"y": ym}
    to_pair = {"c": 1 - c}

    sends, arrivals = {}, {}

    def remote(out_group, in_group, src, dst, dev):
        i = sends.setdefault(out_group, len(sends))
        j = arrivals.setdefault(in_group, len(arrivals))
        return pltpu.make_async_remote_copy(
            src_ref=src,
            dst_ref=dst,
            send_sem=send_sem.at[i],
            recv_sem=recv_sem.at[j],
            device_id=dev,
            device_id_type=MESH_ID,
        )

    def send(out_group, in_group, src, dst, dev):
        remote(out_group, in_group, src, dst, dev).start()

    def arrived(in_group, whole, dev):
        remote(next(iter(sends)), in_group, whole, whole, dev).wait_recv()

    me = y * 2 + c
    wq_own = wq.at[zl, x]
    loads = [
        (0, tok, xg.at[me]),
        (1, qw, wq_own.at[:, pl.ds(0, DK)]),
        (1, kw, wq_own.at[:, pl.ds(DK, DK)]),
        (1, vw, wq_own.at[:, pl.ds(2 * DK, DV)]),
        (1, gw, wq_own.at[:, pl.ds(2 * DK + DV, DV)]),
        (2, ow, wo.at[zl, x]),
        (3, uw, wu.at[zl, x]),
        (4, dw, wd.at[zl, x]),
        (5, gain_mix, gmix),
        (6, gain_mlp, gmlp),
    ]
    for i, src, dst in loads:
        pltpu.make_async_copy(src, dst, local_sem.at[i]).start()

    def decays():
        rt = rate[0]
        i = lax.broadcasted_iota(jnp.int32, (CH, CH), 0)
        j = lax.broadcasted_iota(jnp.int32, (CH, CH), 1)
        near = (i - j).astype(F32)
        for d in range(NCH):
            dist = near + float(d * CH)
            value = jnp.exp(-rt * jnp.maximum(dist, 0.0)) * DK ** (-0.5)
            dec[d] = jnp.where(dist >= 0.0, value, 0.0)

    decays()
    barrier = pltpu.get_barrier_semaphore()
    for dev in (to_xp, to_xm, to_zp, to_zm, to_yp, to_ym, to_pair):
        pl.semaphore_signal(barrier, inc=1, device_id=dev, device_id_type=MESH_ID)
    pl.semaphore_wait(barrier, 7)

    weights = {"q": (wq, 128), "o": (wo, 256), "u": (wu, 128), "d": (wd, 1024)}

    def slab(w, half, first, second, quarter=None):
        buf, n = weights[w]
        start, size = (0 if half == "A" else n // 2), n // 2
        if quarter is not None:
            size //= 2
            start += quarter * size
        zi, xi = (second, first) if half == "A" else (first, second)
        return buf.at[zi, xi, pl.ds(start, size)]

    ring_x = (x, xp, xm, x2, to_xp, to_xm)
    ring_z = (zl, zp, zm, z2, to_zp, to_zm)

    def rings(half):
        return (ring_x, ring_z) if half == "A" else (ring_z, ring_x)

    def shards(w, n):
        buf = weights[w][0]
        return buf.at[0, pl.ds(0, n)]

    def half_shard(w):
        buf, n = weights[w]
        return buf.at[0, 0, pl.ds(0, n // 2)]

    def w1(w, half):
        (at, _, _, _, plus, minus), (here, *_) = rings(half)
        s = slab(w, half, at, here)
        send((w, "first"), (w, half, 1), s, s, plus)
        send((w, "first"), (w, half, 1), s, s, minus)

    def w2(w, half):
        (_, up, dn, _, plus, minus), (here, *_) = rings(half)
        arrived((w, half, 1), shards(w, 1), plus)
        s = slab(w, half, dn, here, 0)
        send((w, "first"), (w, half, 2), s, s, plus)
        s = slab(w, half, up, here, 1)
        send((w, "first"), (w, half, 2), s, s, minus)

    def slabs_of(kind, ring):
        at, up, dn, far, _, _ = ring
        return {"o": [at], "n": [up, dn], "f": [far]}[kind]

    def w3(kind, w, half):
        first, (here, _, _, _, plus, minus) = rings(half)
        if kind == "f":
            arrived((w, half, 2), half_shard(w), first[4])
        for i in slabs_of(kind, first):
            s = slab(w, half, i, here)
            send((w, "third"), (w, half, 3, kind), s, s, plus)
            send((w, "third"), (w, half, 3, kind), s, s, minus)

    def last_group(kind, w, half):
        return (w, half, 4, kind if w == "d" else "all")

    def w4(kind, w, half):
        first, (_, up, dn, _, plus, minus) = rings(half)
        slabs = slabs_of(kind, first)
        arrived((w, half, 3, kind), shards(w, len(slabs)), plus)
        for i in slabs:
            s = slab(w, half, i, dn, 0)
            send((w, "fourth"), last_group(kind, w, half), s, s, plus)
            s = slab(w, half, i, up, 1)
            send((w, "fourth"), last_group(kind, w, half), s, s, minus)

    seen = {}

    def w5(kind, w, half):
        plus = rings(half)[1][4]
        seen[w, half] = seen.get((w, half), 0) + 1
        if w == "d":
            ref = shards(w, 1) if kind == "n" else half_shard(w)
            arrived(last_group(kind, w, half), ref, plus)
        elif seen[w, half] == 3:
            arrived(last_group(kind, w, half), shards(w, 2), plus)

    def rows(r):
        return pl.ds(r * CH, CH)

    blk = lambda yy, cc: yy * 2 + cc
    other = 1 - c

    def part(buf, b, r, half=None):
        if half is None:
            return buf.at[b, pl.ds(r * CH, CH)]
        return buf.at[b, pl.ds(r * CH + half * HC, HC)]

    def g1(tag, buf, r):
        s = part(buf, blk(y, c), r)
        send(tag, (tag, r, 1), s, s, to_yp)
        send(tag, (tag, r, 1), s, s, to_ym)
        send(tag, (tag, r, 3), s, s, to_pair)

    def g2(tag, buf, r):
        arrived((tag, r, 1), buf.at[pl.ds(0, 2), rows(r)], to_yp)
        s = part(buf, blk(ym, c), r, 0)
        send(tag, (tag, r, 2), s, s, to_yp)
        s = part(buf, blk(yp, c), r, 1)
        send(tag, (tag, r, 2), s, s, to_ym)
        s = part(buf, blk(ym, c), r)
        send(tag, (tag, r, 3), s, s, to_pair)
        s = part(buf, blk(yp, c), r)
        send(tag, (tag, r, 3), s, s, to_pair)

    def g3(tag, buf, r):
        s = part(buf, blk(y2, c), r)
        arrived((tag, r, 2), s, to_yp)
        send(tag, (tag, r, 3), s, s, to_pair)

    def g4(tag, buf, r):
        arrived((tag, r, 3), buf.at[pl.ds(0, 4), rows(r)], to_pair)

    def s0(p, r):
        own, snd, prc = sums[p][:3]
        send(("pair", p), (p, r, 0), snd.at[:, rows(r)], prc.at[:, rows(r)], to_pair)

    def pair_sum(p, r, b, lo, n):
        own, snd, prc = sums[p][:3]
        at = pl.ds(r * CH + lo, n)
        return own[b, at, :].astype(F32) + prc[b, at, :].astype(F32)

    def s1(p, r):
        _, _, prc, s_a, s_b, _, _, r_a, r_b, _, _ = sums[p]
        arrived((p, r, 0), prc.at[:, rows(r)], to_pair)
        s_a[r] = pair_sum(p, r, y2, 0, HC).astype(BF16)
        send(("ring", p), (p, r, 1), s_a.at[r], r_a.at[r], to_yp)
        s_b[r] = pair_sum(p, r, y2, HC, HC).astype(BF16)
        send(("ring", p), (p, r, 1), s_b.at[r], r_b.at[r], to_ym)

    def s2(p, r):
        own, _, _, _, _, s_p, s_m, r_a, r_b, r_p, r_m = sums[p]
        s_p[r, pl.ds(HC, HC)] = pair_sum(p, r, yp, HC, HC).astype(BF16)
        s_m[r, pl.ds(0, HC)] = pair_sum(p, r, ym, 0, HC).astype(BF16)
        arrived((p, r, 1), own.at[0, rows(r)], to_yp)
        s_p[r, pl.ds(0, HC)] = (pair_sum(p, r, yp, 0, HC) + r_a[r].astype(F32)).astype(BF16)
        send(("ring", p), (p, r, 2), s_p.at[r], r_p.at[r], to_yp)
        s_m[r, pl.ds(HC, HC)] = (pair_sum(p, r, ym, HC, HC) + r_b[r].astype(F32)).astype(BF16)
        send(("ring", p), (p, r, 2), s_m.at[r], r_m.at[r], to_ym)

    odd = lax.rem(x, 2)
    column = {1: 1 - odd, 2: odd}

    def s3(p, r):
        own, r_p, r_m = sums[p][0], sums[p][9], sums[p][10]
        total = pair_sum(p, r, y, 0, CH)
        arrived((p, r, 2), own.at[pl.ds(0, 2), rows(r)], to_yp)
        total = total + (r_p[r].astype(F32) + r_m[r].astype(F32))
        if p == 0:
            mg[me, rows(r), :] = (xg[me, rows(r), :].astype(F32) + total).astype(BF16)
            return
        mixed = mg[me, rows(r), :]
        mixed = jnp.where(column[p] == 0, mixed[:, :128], mixed[:, 128:]).astype(F32)
        columns = pl.ds(pl.multiple_of(column[p] * 128, 128), 128)
        out[rows(r), columns] = (mixed + total).astype(BF16)

    def norm(src, gain, r):
        def body(i, carry):
            at = pl.ds(pl.multiple_of(r * CH + i * 64, 64), 64)
            square = jnp.zeros((64, DV), F32)
            for b in range(8):
                v = src[b, at, :].astype(F32)
                square = square + v * v
            mean = jnp.sum(square, axis=-1, keepdims=True) * (1.0 / D)
            scale = lax.rsqrt(mean + EPS)
            for b in range(8):
                v = src[b, at, :].astype(F32)
                g = gain[pl.ds(b * DV, DV)].reshape(1, DV).astype(F32)
                nrm[at, b * DV : (b + 1) * DV] = (v * scale * g).astype(BF16)
            return carry

        lax.fori_loop(0, CH // 64, body, 0, unroll=2)

    def dot(a, b):
        return jnp.dot(a, b, preferred_element_type=F32)

    def mixa(r):
        a = nrm[rows(r), :]
        qkv = dot(a, wq[:, :, :, 0 : 2 * DK + DV].reshape(D, 2 * DK + DV))
        q = qkv[:, :DK].astype(BF16)
        kbuf[rows(r), :] = qkv[:, DK : 2 * DK].astype(BF16)
        vbuf[rows(r), :] = qkv[:, 2 * DK :].astype(BF16)
        gate = dot(a, wq[:, :, :, 2 * DK + DV :].reshape(D, DV))
        kept = jnp.zeros((CH, DV), F32)
        for b in range(r + 1):
            score = lax.dot_general(
                q, kbuf[rows(b), :], (((1,), (1,)), ((), ())), preferred_element_type=F32
            )
            score = (score * dec[r - b]).astype(BF16)
            kept = kept + dot(score, vbuf[rows(b), :])
        mean = jnp.mean(kept * kept, axis=-1, keepdims=True)
        kept = kept * lax.rsqrt(mean + EPS)
        hid[rows(r), :] = (gate / (1.0 + jnp.exp(-gate)) * kept).astype(BF16)

    def mix(r):
        own, snd = sums[0][:2]
        for b in range(4):
            for dst, cc in ((snd, other), (own, c)):
                right = jnp.concatenate([wo[b, 2 * cc], wo[b, 2 * cc + 1]], axis=1)
                dst[b, rows(r), :] = dot(hid[rows(r), :], right).astype(BF16)

    def up(r):
        a = nrm[rows(r), :]
        for b in range(4):
            upward = dot(a, wu[:, :, :, b * 256 : (b + 1) * 256].reshape(D, 256))
            upward = jnp.maximum(upward, 0.0)
            act[rows(r), b * 256 : (b + 1) * 256] = (upward * upward).astype(BF16)

    def down(p, r):
        own, snd = sums[p][:2]
        for b in (0, 2):
            for dst, cc in ((snd, other), (own, c)):
                at = 2 * cc + column[p]
                right = jnp.concatenate([wd[b, at], wd[b + 1, at]], axis=1)
                value = dot(act[rows(r), :], right).astype(BF16)
                dst[b, rows(r), :] = value[:, :128]
                dst[b + 1, rows(r), :] = value[:, 128:]

    def load(names):
        own = (xg.at[me], wq_own, wo.at[zl, x], wu.at[zl, x], wd.at[zl, x], gmix, gmlp)
        for i, ref in enumerate(own):
            if "tqoudab"[i] in names:
                pltpu.make_async_copy(ref, ref, local_sem.at[i]).wait()

    feats = {"t": (xg, gmix), "m": (mg, gmlp)}
    kinds = {"w3": w3, "w4": w4, "w5": w5}
    plain = {
        "load": load, "w1": w1, "w2": w2, "s0": s0, "s1": s1, "s2": s2, "s3": s3,
        "mixa": mixa, "mix": mix, "up": up, "down": down,
    }
    gathers = {"g1": g1, "g2": g2, "g3": g3, "g4": g4}
    for name, *args in ORDER:
        if name == "norm":
            norm(*feats[args[0]], args[1])
        elif name in gathers:
            gathers[name](args[0], feats[args[0]][0], args[1])
        elif name in plain:
            plain[name](*args)
        else:
            kinds[name[:2]](name[2], *args)
    def left(out_group, whole):
        remote(out_group, next(iter(arrivals)), whole, whole, to_pair).wait_send()

    for w, (buf, _) in weights.items():
        left((w, "first"), shards(w, 3))
        left((w, "third"), buf.at[pl.ds(0, 2)])
        left((w, "fourth"), shards(w, 4))
    for tag, (buf, _) in feats.items():
        left(tag, buf.at[pl.ds(0, 7)])
    for p in range(3):
        own = sums[p][0]
        left(("pair", p), own)
        left(("ring", p), own.at[pl.ds(0, 3)])


def local(
    tokens, gain_mix, query_weight, key_weight, value_weight, gate_weight,
    decay_rate, out_weight, gain_mlp, up_weight, down_weight,
):
    hbm = pl.BlockSpec(memory_space=pltpu.HBM)
    vmem = pl.BlockSpec(memory_space=pltpu.VMEM)
    smem = pl.BlockSpec(memory_space=pltpu.SMEM)

    def summing(width):
        whole = [pltpu.VMEM((4, SEQ, width), BF16)] * 3
        moved = [pltpu.VMEM((NCH, n, width), BF16) for n in (HC, HC, CH, CH)]
        return whole + moved + moved

    def stay(v):
        return pltpu.with_memory_space_constraint(v, pltpu.HBM)

    return pl.pallas_call(
        kernel,
        out_shape=jax.ShapeDtypeStruct((SEQ, DV), BF16),
        in_specs=[hbm, hbm, hbm, hbm, hbm, hbm, smem, hbm, hbm, hbm, hbm],
        out_specs=vmem,
        scratch_shapes=[
            pltpu.VMEM((D,), BF16),
            pltpu.VMEM((D,), BF16),
            pltpu.VMEM((8, SEQ, DV), BF16),
            pltpu.VMEM((8, SEQ, DV), BF16),
            pltpu.VMEM((SEQ, D), BF16),
            pltpu.VMEM((4, 4, 128, 768), BF16),
            pltpu.VMEM((4, 4, 256, 128), BF16),
            pltpu.VMEM((4, 4, 128, 1024), BF16),
            pltpu.VMEM((4, 4, 1024, 128), BF16),
            pltpu.VMEM((SEQ, DK), BF16),
            pltpu.VMEM((SEQ, DV), BF16),
            pltpu.VMEM((NCH, CH, CH), F32),
            pltpu.VMEM((SEQ, DV), BF16),
            pltpu.VMEM((SEQ, 1024), BF16),
            pltpu.SemaphoreType.DMA((N_SENDS,)),
            pltpu.SemaphoreType.DMA((N_ARRIVALS,)),
            pltpu.SemaphoreType.DMA((N_LOCAL,)),
            *summing(DV), *summing(128), *summing(128),
        ],
        compiler_params=pltpu.CompilerParams(
            collective_id=0, has_side_effects=True, vmem_limit_bytes=52 * 1024 * 1024
        ),
    )(
        stay(tokens), stay(gain_mix), stay(query_weight), stay(key_weight), stay(value_weight),
        stay(gate_weight), decay_rate, stay(out_weight), stay(gain_mlp), stay(up_weight),
        stay(down_weight),
    )


def solution(mesh):
    finer = Mesh(
        mesh.devices.reshape(mesh.shape["rep"], 4, 4, 4, 2), ("rep", "zl", "x", "y", "c")
    )
    placed = (
        P(("rep", "zl", "x"), TP), P(), P(FS, TP), P(FS, TP), P(FS, TP), P(FS, TP),
        P(TP), P(TP, FS), P(), P(FS, TP), P(TP, FS),
    )
    return jax.shard_map(
        local, mesh=finer, in_specs=placed, out_specs=P(("rep", "zl", "x"), TP), check_vma=False
    )
```

```python
import functools

import jax
import jax.numpy as jnp
from jax import lax
from jax.experimental import pallas as pl
from jax.experimental.pallas import tpu as pltpu
from jax.sharding import Mesh
from jax.sharding import PartitionSpec as P

DK = 128
DV = 256
SEQ = 768
D = 2048
CH = 256
NCH = SEQ // CH
HC = CH // 2
EPS = 1e-06
F32 = jnp.float32
BF16 = jnp.bfloat16
TP = ("y", "c")
FS = ("zl", "x")
ORDER = [
    ('load', 'ud'), ('load', 'qkvg'), ('load', 't'), ('w1', 'q', 'B'), ('w1', 'q', 'A'), ('g1', 't', 1),
    ('load', 'o'), ('w1', 'o', 'B'), ('w3o', 'o', 'A'), ('g1', 't', 2), ('w1', 'o', 'A'), ('w3o', 'q', 'B'),
    ('w3o', 'q', 'A'), ('w1', 'u', 'A'), ('g1', 't', 0), ('w3o', 'o', 'B'), ('w1', 'u', 'B'),
    ('w2', 'q', 'A'), ('w2', 'o', 'B'), ('w2', 'o', 'A'), ('w2', 'q', 'B'), ('w3n', 'q', 'A'),
    ('w3n', 'o', 'A'), ('w3n', 'q', 'B'), ('g2', 't', 1), ('g2', 't', 2), ('g2', 't', 0), ('w3f', 'o', 'A'),
    ('w3f', 'q', 'A'), ('g3', 't', 1), ('w4o', 'q', 'A'), ('w4o', 'o', 'B'), ('w4o', 'o', 'A'),
    ('w3f', 'q', 'B'), ('w3f', 'o', 'B'), ('w3n', 'o', 'B'), ('g4', 't', 1), ('w4n', 'q', 'A'),
    ('w4o', 'q', 'B'), ('w4n', 'q', 'B'), ('g3', 't', 2), ('g3', 't', 0), ('load', 'a'), ('norm', 't', 1),
    ('w4f', 'q', 'B'), ('g4', 't', 2), ('g4', 't', 0), ('norm', 't', 0), ('norm', 't', 2), ('w4f', 'q', 'A'),
    ('w4n', 'o', 'B'), ('w5o', 'o', 'A'), ('w4n', 'o', 'A'), ('w4f', 'o', 'A'), ('w4f', 'o', 'B'),
    ('w3o', 'u', 'B'), ('w2', 'u', 'B'), ('w5o', 'q', 'A'), ('w1', 'd', 'B'), ('w5n', 'q', 'B'),
    ('w5f', 'q', 'B'), ('w2', 'u', 'A'), ('w5f', 'q', 'A'), ('w5n', 'q', 'A'), ('w5o', 'o', 'B'),
    ('w3o', 'u', 'A'), ('w5o', 'q', 'B'), ('w1', 'd', 'A'), ('mixa', 0), ('w5n', 'o', 'A'), ('w5n', 'o', 'B'),
    ('w5f', 'o', 'A'), ('w5f', 'o', 'B'), ('mix', 0), ('s0', 0, 0), ('mixa', 1), ('w3n', 'u', 'A'),
    ('mix', 1), ('s0', 0, 1), ('s1', 0, 0), ('w3f', 'u', 'B'), ('mixa', 2), ('mix', 2), ('s0', 0, 2),
    ('s1', 0, 1), ('w3n', 'u', 'B'), ('s1', 0, 2), ('w2', 'd', 'A'), ('s2', 0, 0), ('w2', 'd', 'B'),
    ('s2', 0, 1), ('w4o', 'u', 'B'), ('w3f', 'u', 'A'), ('s2', 0, 2), ('s3', 0, 0), ('g1', 'm', 0),
    ('w4n', 'u', 'A'), ('w3n', 'd', 'A'), ('w3n', 'd', 'B'), ('w4f', 'u', 'B'), ('w4f', 'u', 'A'),
    ('w5o', 'u', 'B'), ('w4o', 'u', 'A'), ('s3', 0, 2), ('g1', 'm', 2), ('w4n', 'u', 'B'), ('w3o', 'd', 'A'),
    ('s3', 0, 1), ('g2', 'm', 0), ('g1', 'm', 1), ('w3f', 'd', 'B'), ('w3o', 'd', 'B'), ('g2', 'm', 2),
    ('w4n', 'd', 'A'), ('w5n', 'u', 'A'), ('w5f', 'u', 'A'), ('w3f', 'd', 'A'), ('g3', 'm', 0),
    ('g2', 'm', 1), ('w5n', 'u', 'B'), ('g4', 'm', 0), ('load', 'b'), ('norm', 'm', 0), ('w4n', 'd', 'B'),
    ('w5f', 'u', 'B'), ('w5o', 'u', 'A'), ('g3', 'm', 2), ('up', 0), ('w4f', 'd', 'B'), ('w4o', 'd', 'A'),
    ('g4', 'm', 2), ('norm', 'm', 2), ('up', 2), ('g3', 'm', 1), ('w5n', 'd', 'A'), ('w4o', 'd', 'B'),
    ('down', 1, 2), ('s0', 1, 2), ('down', 1, 0), ('s0', 1, 0), ('g4', 'm', 1), ('s1', 1, 2),
    ('norm', 'm', 1), ('w4f', 'd', 'A'), ('s1', 1, 0), ('up', 1), ('down', 1, 1), ('w5f', 'd', 'B'),
    ('s0', 1, 1), ('s2', 1, 2), ('s1', 1, 1), ('w5o', 'd', 'A'), ('w5n', 'd', 'B'), ('w5o', 'd', 'B'),
    ('s2', 1, 0), ('w5f', 'd', 'A'), ('down', 2, 2), ('s0', 2, 2), ('down', 2, 1), ('s0', 2, 1), ('s1', 2, 2),
    ('down', 2, 0), ('s1', 2, 1), ('s3', 1, 2), ('s0', 2, 0), ('s2', 1, 1), ('s1', 2, 0), ('s2', 2, 2),
    ('s3', 1, 0), ('s2', 2, 1), ('s3', 1, 1), ('s2', 2, 0), ('s3', 2, 1), ('s3', 2, 2), ('s3', 2, 0),
]
MESH_ID = pl.DeviceIdType.MESH
N_SENDS = 20
N_ARRIVALS = 97
N_LOCAL = 7


def kernel(
    tok, gain_mix, qw, kw, vw, gw, rate, ow, gain_mlp, uw, dw,
    out,
    gmix, gmlp, xg, mg, nrm, wq, wo, wu, wd, kbuf, vbuf, dec, hid, act,
    send_sem, recv_sem, local_sem, *summing,
):
    sums = [summing[11 * p : 11 * p + 11] for p in range(3)]
    rep, zl = lax.axis_index("rep"), lax.axis_index("zl")
    x, y, c = lax.axis_index("x"), lax.axis_index("y"), lax.axis_index("c")

    def mod4(v):
        return lax.rem(v + 4, 4)

    def z_id(step):
        z = lax.rem(rep * 4 + zl + step + 8, 8)
        return {"rep": z // 4, "zl": lax.rem(z, 4)}

    xp, xm, x2 = mod4(x + 1), mod4(x - 1), mod4(x + 2)
    zp, zm, z2 = mod4(zl + 1), mod4(zl - 1), mod4(zl + 2)
    yp, ym, y2 = mod4(y + 1), mod4(y - 1), mod4(y + 2)
    to_xp, to_xm = {"x": xp}, {"x": xm}
    to_zp, to_zm = z_id(1), z_id(-1)
    to_yp, to_ym = {"y": yp}, {"y": ym}
    to_pair = {"c": 1 - c}

    sends, arrivals = {}, {}

    def remote(out_group, in_group, src, dst, dev):
        i = sends.setdefault(out_group, len(sends))
        j = arrivals.setdefault(in_group, len(arrivals))
        return pltpu.make_async_remote_copy(
            src_ref=src,
            dst_ref=dst,
            send_sem=send_sem.at[i],
            recv_sem=recv_sem.at[j],
            device_id=dev,
            device_id_type=MESH_ID,
        )

    def send(out_group, in_group, src, dst, dev):
        remote(out_group, in_group, src, dst, dev).start()

    def arrived(in_group, whole, dev):
        remote(next(iter(sends)), in_group, whole, whole, dev).wait_recv()

    me = y * 2 + c
    wq_own = wq.at[zl, x]
    loads = [
        (0, tok, xg.at[me]),
        (1, qw, wq_own.at[:, pl.ds(0, DK)]),
        (1, kw, wq_own.at[:, pl.ds(DK, DK)]),
        (1, vw, wq_own.at[:, pl.ds(2 * DK, DV)]),
        (1, gw, wq_own.at[:, pl.ds(2 * DK + DV, DV)]),
        (2, ow, wo.at[zl, x]),
        (3, uw, wu.at[zl, x]),
        (4, dw, wd.at[zl, x]),
        (5, gain_mix, gmix),
        (6, gain_mlp, gmlp),
    ]
    for i, src, dst in loads:
        pltpu.make_async_copy(src, dst, local_sem.at[i]).start()

    def decays():
        rt = rate[0]
        i = lax.broadcasted_iota(jnp.int32, (CH, CH), 0)
        j = lax.broadcasted_iota(jnp.int32, (CH, CH), 1)
        near = (i - j).astype(F32)
        for d in range(NCH):
            dist = near + float(d * CH)
            value = jnp.exp(-rt * jnp.maximum(dist, 0.0)) * DK ** (-0.5)
            dec[d] = jnp.where(dist >= 0.0, value, 0.0)

    decays()
    barrier = pltpu.get_barrier_semaphore()
    for dev in (to_xp, to_xm, to_zp, to_zm, to_yp, to_ym, to_pair):
        pl.semaphore_signal(barrier, inc=1, device_id=dev, device_id_type=MESH_ID)
    pl.semaphore_wait(barrier, 7)

    weights = {"q": (wq, 128), "o": (wo, 256), "u": (wu, 128), "d": (wd, 1024)}

    def slab(w, half, first, second, quarter=None):
        buf, n = weights[w]
        start, size = (0 if half == "A" else n // 2), n // 2
        if quarter is not None:
            size //= 2
            start += quarter * size
        zi, xi = (second, first) if half == "A" else (first, second)
        return buf.at[zi, xi, pl.ds(start, size)]

    ring_x = (x, xp, xm, x2, to_xp, to_xm)
    ring_z = (zl, zp, zm, z2, to_zp, to_zm)

    def rings(half):
        return (ring_x, ring_z) if half == "A" else (ring_z, ring_x)

    def shards(w, n):
        buf = weights[w][0]
        return buf.at[0, pl.ds(0, n)]

    def half_shard(w):
        buf, n = weights[w]
        return buf.at[0, 0, pl.ds(0, n // 2)]

    def w1(w, half):
        (at, _, _, _, plus, minus), (here, *_) = rings(half)
        s = slab(w, half, at, here)
        send((w, "first"), (w, half, 1), s, s, plus)
        send((w, "first"), (w, half, 1), s, s, minus)

    def w2(w, half):
        (_, up, dn, _, plus, minus), (here, *_) = rings(half)
        arrived((w, half, 1), shards(w, 1), plus)
        s = slab(w, half, dn, here, 0)
        send((w, "first"), (w, half, 2), s, s, plus)
        s = slab(w, half, up, here, 1)
        send((w, "first"), (w, half, 2), s, s, minus)

    def slabs_of(kind, ring):
        at, up, dn, far, _, _ = ring
        return {"o": [at], "n": [up, dn], "f": [far]}[kind]

    def w3(kind, w, half):
        first, (here, _, _, _, plus, minus) = rings(half)
        if kind == "f":
            arrived((w, half, 2), half_shard(w), first[4])
        for i in slabs_of(kind, first):
            s = slab(w, half, i, here)
            send((w, "third"), (w, half, 3, kind), s, s, plus)
            send((w, "third"), (w, half, 3, kind), s, s, minus)

    def last_group(kind, w, half):
        return (w, half, 4, kind if w == "d" else "all")

    def w4(kind, w, half):
        first, (_, up, dn, _, plus, minus) = rings(half)
        slabs = slabs_of(kind, first)
        arrived((w, half, 3, kind), shards(w, len(slabs)), plus)
        for i in slabs:
            s = slab(w, half, i, dn, 0)
            send((w, "fourth"), last_group(kind, w, half), s, s, plus)
            s = slab(w, half, i, up, 1)
            send((w, "fourth"), last_group(kind, w, half), s, s, minus)

    seen = {}

    def w5(kind, w, half):
        plus = rings(half)[1][4]
        seen[w, half] = seen.get((w, half), 0) + 1
        if w == "d":
            ref = shards(w, 1) if kind == "n" else half_shard(w)
            arrived(last_group(kind, w, half), ref, plus)
        elif seen[w, half] == 3:
            arrived(last_group(kind, w, half), shards(w, 2), plus)

    def rows(r):
        return pl.ds(r * CH, CH)

    blk = lambda yy, cc: yy * 2 + cc
    other = 1 - c

    def part(buf, b, r, half=None):
        if half is None:
            return buf.at[b, pl.ds(r * CH, CH)]
        return buf.at[b, pl.ds(r * CH + half * HC, HC)]

    def g1(tag, buf, r):
        s = part(buf, blk(y, c), r)
        send(tag, (tag, r, 1), s, s, to_yp)
        send(tag, (tag, r, 1), s, s, to_ym)
        send(tag, (tag, r, 3), s, s, to_pair)

    def g2(tag, buf, r):
        arrived((tag, r, 1), buf.at[pl.ds(0, 2), rows(r)], to_yp)
        s = part(buf, blk(ym, c), r, 0)
        send(tag, (tag, r, 2), s, s, to_yp)
        s = part(buf, blk(yp, c), r, 1)
        send(tag, (tag, r, 2), s, s, to_ym)
        s = part(buf, blk(ym, c), r)
        send(tag, (tag, r, 3), s, s, to_pair)
        s = part(buf, blk(yp, c), r)
        send(tag, (tag, r, 3), s, s, to_pair)

    def g3(tag, buf, r):
        s = part(buf, blk(y2, c), r)
        arrived((tag, r, 2), s, to_yp)
        send(tag, (tag, r, 3), s, s, to_pair)

    def g4(tag, buf, r):
        arrived((tag, r, 3), buf.at[pl.ds(0, 4), rows(r)], to_pair)

    def s0(p, r):
        own, snd, prc = sums[p][:3]
        send(("pair", p), (p, r, 0), snd.at[:, rows(r)], prc.at[:, rows(r)], to_pair)

    def pair_sum(p, r, b, lo, n):
        own, snd, prc = sums[p][:3]
        at = pl.ds(r * CH + lo, n)
        return own[b, at, :].astype(F32) + prc[b, at, :].astype(F32)

    def s1(p, r):
        _, _, prc, s_a, s_b, _, _, r_a, r_b, _, _ = sums[p]
        arrived((p, r, 0), prc.at[:, rows(r)], to_pair)
        s_a[r] = pair_sum(p, r, y2, 0, HC).astype(BF16)
        send(("ring", p), (p, r, 1), s_a.at[r], r_a.at[r], to_yp)
        s_b[r] = pair_sum(p, r, y2, HC, HC).astype(BF16)
        send(("ring", p), (p, r, 1), s_b.at[r], r_b.at[r], to_ym)

    def s2(p, r):
        own, _, _, _, _, s_p, s_m, r_a, r_b, r_p, r_m = sums[p]
        s_p[r, pl.ds(HC, HC)] = pair_sum(p, r, yp, HC, HC).astype(BF16)
        s_m[r, pl.ds(0, HC)] = pair_sum(p, r, ym, 0, HC).astype(BF16)
        arrived((p, r, 1), own.at[0, rows(r)], to_yp)
        s_p[r, pl.ds(0, HC)] = (pair_sum(p, r, yp, 0, HC) + r_a[r].astype(F32)).astype(BF16)
        send(("ring", p), (p, r, 2), s_p.at[r], r_p.at[r], to_yp)
        s_m[r, pl.ds(HC, HC)] = (pair_sum(p, r, ym, HC, HC) + r_b[r].astype(F32)).astype(BF16)
        send(("ring", p), (p, r, 2), s_m.at[r], r_m.at[r], to_ym)

    odd = lax.rem(x, 2)
    column = {1: 1 - odd, 2: odd}

    def s3(p, r):
        own, r_p, r_m = sums[p][0], sums[p][9], sums[p][10]
        total = pair_sum(p, r, y, 0, CH)
        arrived((p, r, 2), own.at[pl.ds(0, 2), rows(r)], to_yp)
        total = total + (r_p[r].astype(F32) + r_m[r].astype(F32))
        if p == 0:
            mg[me, rows(r), :] = (xg[me, rows(r), :].astype(F32) + total).astype(BF16)
            return
        mixed = mg[me, rows(r), :]
        mixed = jnp.where(column[p] == 0, mixed[:, :128], mixed[:, 128:]).astype(F32)
        columns = pl.ds(pl.multiple_of(column[p] * 128, 128), 128)
        out[rows(r), columns] = (mixed + total).astype(BF16)

    def norm(src, gain, r):
        def body(i, carry):
            at = pl.ds(pl.multiple_of(r * CH + i * 64, 64), 64)
            square = jnp.zeros((64, DV), F32)
            for b in range(8):
                v = src[b, at, :].astype(F32)
                square = square + v * v
            mean = jnp.sum(square, axis=-1, keepdims=True) * (1.0 / D)
            scale = lax.rsqrt(mean + EPS)
            for b in range(8):
                v = src[b, at, :].astype(F32)
                g = gain[pl.ds(b * DV, DV)].reshape(1, DV).astype(F32)
                nrm[at, b * DV : (b + 1) * DV] = (v * scale * g).astype(BF16)
            return carry

        lax.fori_loop(0, CH // 64, body, 0, unroll=2)

    def dot(a, b):
        return jnp.dot(a, b, preferred_element_type=F32)

    def mixa(r):
        a = nrm[rows(r), :]
        qkv = dot(a, wq[:, :, :, 0 : 2 * DK + DV].reshape(D, 2 * DK + DV))
        q = qkv[:, :DK].astype(BF16)
        kbuf[rows(r), :] = qkv[:, DK : 2 * DK].astype(BF16)
        vbuf[rows(r), :] = qkv[:, 2 * DK :].astype(BF16)
        gate = dot(a, wq[:, :, :, 2 * DK + DV :].reshape(D, DV))
        kept = jnp.zeros((CH, DV), F32)
        for b in range(r + 1):
            score = lax.dot_general(
                q, kbuf[rows(b), :], (((1,), (1,)), ((), ())), preferred_element_type=F32
            )
            score = (score * dec[r - b]).astype(BF16)
            kept = kept + dot(score, vbuf[rows(b), :])
        mean = jnp.mean(kept * kept, axis=-1, keepdims=True)
        kept = kept * lax.rsqrt(mean + EPS)
        hid[rows(r), :] = (gate / (1.0 + jnp.exp(-gate)) * kept).astype(BF16)

    def mix(r):
        own, snd = sums[0][:2]
        for b in range(4):
            for dst, cc in ((snd, other), (own, c)):
                right = jnp.concatenate([wo[b, 2 * cc], wo[b, 2 * cc + 1]], axis=1)
                dst[b, rows(r), :] = dot(hid[rows(r), :], right).astype(BF16)

    def up(r):
        a = nrm[rows(r), :]
        for b in range(4):
            upward = dot(a, wu[:, :, :, b * 256 : (b + 1) * 256].reshape(D, 256))
            upward = jnp.maximum(upward, 0.0)
            act[rows(r), b * 256 : (b + 1) * 256] = (upward * upward).astype(BF16)

    def down(p, r):
        own, snd = sums[p][:2]
        for b in (0, 2):
            for dst, cc in ((snd, other), (own, c)):
                at = 2 * cc + column[p]
                right = jnp.concatenate([wd[b, at], wd[b + 1, at]], axis=1)
                value = dot(act[rows(r), :], right).astype(BF16)
                dst[b, rows(r), :] = value[:, :128]
                dst[b + 1, rows(r), :] = value[:, 128:]

    def load(names):
        own = (xg.at[me], wq_own, wo.at[zl, x], wu.at[zl, x], wd.at[zl, x], gmix, gmlp)
        for i, ref in enumerate(own):
            if "tqoudab"[i] in names:
                pltpu.make_async_copy(ref, ref, local_sem.at[i]).wait()

    feats = {"t": (xg, gmix), "m": (mg, gmlp)}
    kinds = {"w3": w3, "w4": w4, "w5": w5}
    plain = {
        "load": load, "w1": w1, "w2": w2, "s0": s0, "s1": s1, "s2": s2, "s3": s3,
        "mixa": mixa, "mix": mix, "up": up, "down": down,
    }
    gathers = {"g1": g1, "g2": g2, "g3": g3, "g4": g4}
    for name, *args in ORDER:
        if name == "norm":
            norm(*feats[args[0]], args[1])
        elif name in gathers:
            gathers[name](args[0], feats[args[0]][0], args[1])
        elif name in plain:
            plain[name](*args)
        else:
            kinds[name[:2]](name[2], *args)
    def left(out_group, whole):
        remote(out_group, next(iter(arrivals)), whole, whole, to_pair).wait_send()

    for w, (buf, _) in weights.items():
        left((w, "first"), shards(w, 3))
        left((w, "third"), buf.at[pl.ds(0, 2)])
        left((w, "fourth"), shards(w, 4))
    for tag, (buf, _) in feats.items():
        left(tag, buf.at[pl.ds(0, 7)])
    for p in range(3):
        own = sums[p][0]
        left(("pair", p), own)
        left(("ring", p), own.at[pl.ds(0, 3)])


def local(
    tokens, gain_mix, query_weight, key_weight, value_weight, gate_weight,
    decay_rate, out_weight, gain_mlp, up_weight, down_weight,
):
    hbm = pl.BlockSpec(memory_space=pltpu.HBM)
    vmem = pl.BlockSpec(memory_space=pltpu.VMEM)
    smem = pl.BlockSpec(memory_space=pltpu.SMEM)

    def summing(width):
        whole = [pltpu.VMEM((4, SEQ, width), BF16)] * 3
        moved = [pltpu.VMEM((NCH, n, width), BF16) for n in (HC, HC, CH, CH)]
        return whole + moved + moved

    def stay(v):
        return pltpu.with_memory_space_constraint(v, pltpu.HBM)

    return pl.pallas_call(
        kernel,
        out_shape=jax.ShapeDtypeStruct((SEQ, DV), BF16),
        in_specs=[hbm, hbm, hbm, hbm, hbm, hbm, smem, hbm, hbm, hbm, hbm],
        out_specs=vmem,
        scratch_shapes=[
            pltpu.VMEM((D,), BF16),
            pltpu.VMEM((D,), BF16),
            pltpu.VMEM((8, SEQ, DV), BF16),
            pltpu.VMEM((8, SEQ, DV), BF16),
            pltpu.VMEM((SEQ, D), BF16),
            pltpu.VMEM((4, 4, 128, 768), BF16),
            pltpu.VMEM((4, 4, 256, 128), BF16),
            pltpu.VMEM((4, 4, 128, 1024), BF16),
            pltpu.VMEM((4, 4, 1024, 128), BF16),
            pltpu.VMEM((SEQ, DK), BF16),
            pltpu.VMEM((SEQ, DV), BF16),
            pltpu.VMEM((NCH, CH, CH), F32),
            pltpu.VMEM((SEQ, DV), BF16),
            pltpu.VMEM((SEQ, 1024), BF16),
            pltpu.SemaphoreType.DMA((N_SENDS,)),
            pltpu.SemaphoreType.DMA((N_ARRIVALS,)),
            pltpu.SemaphoreType.DMA((N_LOCAL,)),
            *summing(DV), *summing(128), *summing(128),
        ],
        compiler_params=pltpu.CompilerParams(
            collective_id=0, has_side_effects=True, vmem_limit_bytes=52 * 1024 * 1024
        ),
    )(
        stay(tokens), stay(gain_mix), stay(query_weight), stay(key_weight), stay(value_weight),
        stay(gate_weight), decay_rate, stay(out_weight), stay(gain_mlp), stay(up_weight),
        stay(down_weight),
    )


def solution(mesh):
    finer = Mesh(
        mesh.devices.reshape(mesh.shape["rep"], 4, 4, 4, 2), ("rep", "zl", "x", "y", "c")
    )
    placed = (
        P(("rep", "zl", "x"), TP), P(), P(FS, TP), P(FS, TP), P(FS, TP), P(FS, TP),
        P(TP), P(TP, FS), P(), P(FS, TP), P(TP, FS),
    )
    return jax.shard_map(
        local, mesh=finer, in_specs=placed, out_specs=P(("rep", "zl", "x"), TP), check_vma=False
    )
```

```python
import functools

import jax
import jax.numpy as jnp
from jax import lax
from jax.experimental import pallas as pl
from jax.experimental.pallas import tpu as pltpu
from jax.sharding import Mesh
from jax.sharding import PartitionSpec as P

DK = 128
DV = 256
SEQ = 768
D = 2048
CH = 256
NCH = SEQ // CH
HC = CH // 2
EPS = 1e-06
F32 = jnp.float32
BF16 = jnp.bfloat16
TP = ("y", "c")
FS = ("zl", "x")
ORDER = [
    ('load', 'ud'), ('load', 'qkvg'), ('load', 't'), ('w1', 'q', 'B'), ('w1', 'q', 'A'), ('g1', 't', 1),
    ('load', 'o'), ('w1', 'o', 'B'), ('w3o', 'o', 'A'), ('g1', 't', 2), ('w1', 'o', 'A'), ('w3o', 'q', 'B'),
    ('w3o', 'q', 'A'), ('w1', 'u', 'A'), ('g1', 't', 0), ('w3o', 'o', 'B'), ('w1', 'u', 'B'),
    ('w2', 'q', 'A'), ('w2', 'o', 'B'), ('w2', 'o', 'A'), ('w2', 'q', 'B'), ('w3n', 'q', 'A'),
    ('w3n', 'o', 'A'), ('w3n', 'q', 'B'), ('g2', 't', 1), ('g2', 't', 2), ('g2', 't', 0), ('w3f', 'o', 'A'),
    ('w3f', 'q', 'A'), ('g3', 't', 1), ('w4o', 'q', 'A'), ('w4o', 'o', 'B'), ('w4o', 'o', 'A'),
    ('w3f', 'q', 'B'), ('w3f', 'o', 'B'), ('w3n', 'o', 'B'), ('g4', 't', 1), ('w4n', 'q', 'A'),
    ('w4o', 'q', 'B'), ('w4n', 'q', 'B'), ('g3', 't', 2), ('g3', 't', 0), ('load', 'a'), ('norm', 't', 1),
    ('w4f', 'q', 'B'), ('g4', 't', 2), ('g4', 't', 0), ('norm', 't', 0), ('norm', 't', 2), ('w4f', 'q', 'A'),
    ('w4n', 'o', 'B'), ('w5o', 'o', 'A'), ('w4n', 'o', 'A'), ('w4f', 'o', 'A'), ('w4f', 'o', 'B'),
    ('w3o', 'u', 'B'), ('w2', 'u', 'B'), ('w5o', 'q', 'A'), ('w1', 'd', 'B'), ('w5n', 'q', 'B'),
    ('w5f', 'q', 'B'), ('w2', 'u', 'A'), ('w5f', 'q', 'A'), ('w5n', 'q', 'A'), ('w5o', 'o', 'B'),
    ('w3o', 'u', 'A'), ('w5o', 'q', 'B'), ('w1', 'd', 'A'), ('mixa', 0), ('w5n', 'o', 'A'), ('w5n', 'o', 'B'),
    ('w5f', 'o', 'A'), ('w5f', 'o', 'B'), ('mix', 0), ('mixa', 1), ('w3n', 'u', 'A'), ('mix', 1),
    ('s1', 0, 0), ('w3f', 'u', 'B'), ('mixa', 2), ('mix', 2), ('s1', 0, 1), ('w3n', 'u', 'B'), ('s1', 0, 2),
    ('w2', 'd', 'A'), ('s2', 0, 0), ('w2', 'd', 'B'), ('s2', 0, 1), ('w4o', 'u', 'B'), ('w3f', 'u', 'A'),
    ('s2', 0, 2), ('s3', 0, 0), ('g1', 'm', 0), ('w4n', 'u', 'A'), ('w3n', 'd', 'A'), ('w3n', 'd', 'B'),
    ('w4f', 'u', 'B'), ('w4f', 'u', 'A'), ('w5o', 'u', 'B'), ('w4o', 'u', 'A'), ('s3', 0, 2), ('g1', 'm', 2),
    ('w4n', 'u', 'B'), ('w3o', 'd', 'A'), ('s3', 0, 1), ('g2', 'm', 0), ('g1', 'm', 1), ('w3f', 'd', 'B'),
    ('w3o', 'd', 'B'), ('g2', 'm', 2), ('w4n', 'd', 'A'), ('w5n', 'u', 'A'), ('w5f', 'u', 'A'),
    ('w3f', 'd', 'A'), ('g3', 'm', 0), ('g2', 'm', 1), ('w5n', 'u', 'B'), ('g4', 'm', 0), ('load', 'b'),
    ('norm', 'm', 0), ('w4n', 'd', 'B'), ('w5f', 'u', 'B'), ('w5o', 'u', 'A'), ('g3', 'm', 2), ('up', 0),
    ('w4f', 'd', 'B'), ('w4o', 'd', 'A'), ('g4', 'm', 2), ('norm', 'm', 2), ('up', 2), ('g3', 'm', 1),
    ('w5n', 'd', 'A'), ('w4o', 'd', 'B'), ('down', 1, 2), ('down', 1, 0), ('g4', 'm', 1), ('s1', 1, 2),
    ('norm', 'm', 1), ('w4f', 'd', 'A'), ('s1', 1, 0), ('up', 1), ('down', 1, 1), ('w5f', 'd', 'B'),
    ('s2', 1, 2), ('s1', 1, 1), ('w5o', 'd', 'A'), ('w5n', 'd', 'B'), ('w5o', 'd', 'B'), ('s2', 1, 0),
    ('w5f', 'd', 'A'), ('down', 2, 2), ('down', 2, 1), ('s1', 2, 2), ('down', 2, 0), ('s1', 2, 1),
    ('s3', 1, 2), ('s2', 1, 1), ('s1', 2, 0), ('s2', 2, 2), ('s3', 1, 0), ('s2', 2, 1), ('s3', 1, 1),
    ('s2', 2, 0), ('s3', 2, 1), ('s3', 2, 2), ('s3', 2, 0),
]
MESH_ID = pl.DeviceIdType.MESH
N_SENDS = 20
N_ARRIVALS = 97
N_LOCAL = 7


def kernel(
    tok, gain_mix, qw, kw, vw, gw, rate, ow, gain_mlp, uw, dw,
    out,
    gmix, gmlp, xg, mg, nrm, wq, wo, wu, wd, kbuf, vbuf, dec, hid, act,
    send_sem, recv_sem, local_sem, *summing,
):
    sums = [summing[11 * p : 11 * p + 11] for p in range(3)]
    rep, zl = lax.axis_index("rep"), lax.axis_index("zl")
    x, y, c = lax.axis_index("x"), lax.axis_index("y"), lax.axis_index("c")

    def mod4(v):
        return lax.rem(v + 4, 4)

    def z_id(step):
        z = lax.rem(rep * 4 + zl + step + 8, 8)
        return {"rep": z // 4, "zl": lax.rem(z, 4)}

    xp, xm, x2 = mod4(x + 1), mod4(x - 1), mod4(x + 2)
    zp, zm, z2 = mod4(zl + 1), mod4(zl - 1), mod4(zl + 2)
    yp, ym, y2 = mod4(y + 1), mod4(y - 1), mod4(y + 2)
    to_xp, to_xm = {"x": xp}, {"x": xm}
    to_zp, to_zm = z_id(1), z_id(-1)
    to_yp, to_ym = {"y": yp}, {"y": ym}
    to_pair = {"c": 1 - c}

    sends, arrivals = {}, {}

    def remote(out_group, in_group, src, dst, dev):
        i = sends.setdefault(out_group, len(sends))
        j = arrivals.setdefault(in_group, len(arrivals))
        return pltpu.make_async_remote_copy(
            src_ref=src,
            dst_ref=dst,
            send_sem=send_sem.at[i],
            recv_sem=recv_sem.at[j],
            device_id=dev,
            device_id_type=MESH_ID,
        )

    def send(out_group, in_group, src, dst, dev):
        remote(out_group, in_group, src, dst, dev).start()

    def arrived(in_group, whole, dev):
        remote(next(iter(sends)), in_group, whole, whole, dev).wait_recv()

    me = y * 2 + c
    wq_own = wq.at[zl, x]
    loads = [
        (0, tok, xg.at[me]),
        (1, qw, wq_own.at[:, pl.ds(0, DK)]),
        (1, kw, wq_own.at[:, pl.ds(DK, DK)]),
        (1, vw, wq_own.at[:, pl.ds(2 * DK, DV)]),
        (1, gw, wq_own.at[:, pl.ds(2 * DK + DV, DV)]),
        (2, ow, wo.at[zl, x]),
        (3, uw, wu.at[zl, x]),
        (4, dw, wd.at[zl, x]),
        (5, gain_mix, gmix),
        (6, gain_mlp, gmlp),
    ]
    for i, src, dst in loads:
        pltpu.make_async_copy(src, dst, local_sem.at[i]).start()

    def decays():
        rt = rate[0]
        i = lax.broadcasted_iota(jnp.int32, (CH, CH), 0)
        j = lax.broadcasted_iota(jnp.int32, (CH, CH), 1)
        near = (i - j).astype(F32)
        for d in range(NCH):
            dist = near + float(d * CH)
            value = jnp.exp(-rt * jnp.maximum(dist, 0.0)) * DK ** (-0.5)
            dec[d] = jnp.where(dist >= 0.0, value, 0.0)

    decays()
    barrier = pltpu.get_barrier_semaphore()
    for dev in (to_xp, to_xm, to_zp, to_zm, to_yp, to_ym, to_pair):
        pl.semaphore_signal(barrier, inc=1, device_id=dev, device_id_type=MESH_ID)
    pl.semaphore_wait(barrier, 7)

    weights = {"q": (wq, 128), "o": (wo, 256), "u": (wu, 128), "d": (wd, 1024)}

    def slab(w, half, first, second, quarter=None):
        buf, n = weights[w]
        start, size = (0 if half == "A" else n // 2), n // 2
        if quarter is not None:
            size //= 2
            start += quarter * size
        zi, xi = (second, first) if half == "A" else (first, second)
        return buf.at[zi, xi, pl.ds(start, size)]

    ring_x = (x, xp, xm, x2, to_xp, to_xm)
    ring_z = (zl, zp, zm, z2, to_zp, to_zm)

    def rings(half):
        return (ring_x, ring_z) if half == "A" else (ring_z, ring_x)

    def shards(w, n):
        buf = weights[w][0]
        return buf.at[0, pl.ds(0, n)]

    def half_shard(w):
        buf, n = weights[w]
        return buf.at[0, 0, pl.ds(0, n // 2)]

    def w1(w, half):
        (at, _, _, _, plus, minus), (here, *_) = rings(half)
        s = slab(w, half, at, here)
        send((w, "first"), (w, half, 1), s, s, plus)
        send((w, "first"), (w, half, 1), s, s, minus)

    def w2(w, half):
        (_, up, dn, _, plus, minus), (here, *_) = rings(half)
        arrived((w, half, 1), shards(w, 1), plus)
        s = slab(w, half, dn, here, 0)
        send((w, "first"), (w, half, 2), s, s, plus)
        s = slab(w, half, up, here, 1)
        send((w, "first"), (w, half, 2), s, s, minus)

    def slabs_of(kind, ring):
        at, up, dn, far, _, _ = ring
        return {"o": [at], "n": [up, dn], "f": [far]}[kind]

    def w3(kind, w, half):
        first, (here, _, _, _, plus, minus) = rings(half)
        if kind == "f":
            arrived((w, half, 2), half_shard(w), first[4])
        for i in slabs_of(kind, first):
            s = slab(w, half, i, here)
            send((w, "third"), (w, half, 3, kind), s, s, plus)
            send((w, "third"), (w, half, 3, kind), s, s, minus)

    def last_group(kind, w, half):
        return (w, half, 4, kind if w == "d" else "all")

    def w4(kind, w, half):
        first, (_, up, dn, _, plus, minus) = rings(half)
        slabs = slabs_of(kind, first)
        arrived((w, half, 3, kind), shards(w, len(slabs)), plus)
        for i in slabs:
            s = slab(w, half, i, dn, 0)
            send((w, "fourth"), last_group(kind, w, half), s, s, plus)
            s = slab(w, half, i, up, 1)
            send((w, "fourth"), last_group(kind, w, half), s, s, minus)

    seen = {}

    def w5(kind, w, half):
        plus = rings(half)[1][4]
        seen[w, half] = seen.get((w, half), 0) + 1
        if w == "d":
            ref = shards(w, 1) if kind == "n" else half_shard(w)
            arrived(last_group(kind, w, half), ref, plus)
        elif seen[w, half] == 3:
            arrived(last_group(kind, w, half), shards(w, 2), plus)

    def rows(r):
        return pl.ds(r * CH, CH)

    blk = lambda yy, cc: yy * 2 + cc
    other = 1 - c

    def part(buf, b, r, half=None):
        if half is None:
            return buf.at[b, pl.ds(r * CH, CH)]
        return buf.at[b, pl.ds(r * CH + half * HC, HC)]

    def g1(tag, buf, r):
        s = part(buf, blk(y, c), r)
        send(tag, (tag, r, 1), s, s, to_yp)
        send(tag, (tag, r, 1), s, s, to_ym)
        send(tag, (tag, r, 3), s, s, to_pair)

    def g2(tag, buf, r):
        arrived((tag, r, 1), buf.at[pl.ds(0, 2), rows(r)], to_yp)
        s = part(buf, blk(ym, c), r, 0)
        send(tag, (tag, r, 2), s, s, to_yp)
        s = part(buf, blk(yp, c), r, 1)
        send(tag, (tag, r, 2), s, s, to_ym)
        s = part(buf, blk(ym, c), r)
        send(tag, (tag, r, 3), s, s, to_pair)
        s = part(buf, blk(yp, c), r)
        send(tag, (tag, r, 3), s, s, to_pair)

    def g3(tag, buf, r):
        s = part(buf, blk(y2, c), r)
        arrived((tag, r, 2), s, to_yp)
        send(tag, (tag, r, 3), s, s, to_pair)

    def g4(tag, buf, r):
        arrived((tag, r, 3), buf.at[pl.ds(0, 4), rows(r)], to_pair)

    def s0(p, r):
        own, snd, prc = sums[p][:3]
        send(("pair", p), (p, r, 0), snd.at[:, rows(r)], prc.at[:, rows(r)], to_pair)

    def pair_sum(p, r, b, lo, n):
        own, snd, prc = sums[p][:3]
        at = pl.ds(r * CH + lo, n)
        return own[b, at, :].astype(F32) + prc[b, at, :].astype(F32)

    def s1(p, r):
        _, _, prc, s_a, s_b, _, _, r_a, r_b, _, _ = sums[p]
        arrived((p, r, 0), prc.at[:, rows(r)], to_pair)
        s_a[r] = pair_sum(p, r, y2, 0, HC).astype(BF16)
        send(("ring", p), (p, r, 1), s_a.at[r], r_a.at[r], to_yp)
        s_b[r] = pair_sum(p, r, y2, HC, HC).astype(BF16)
        send(("ring", p), (p, r, 1), s_b.at[r], r_b.at[r], to_ym)

    def s2(p, r):
        own, _, _, _, _, s_p, s_m, r_a, r_b, r_p, r_m = sums[p]
        s_p[r, pl.ds(HC, HC)] = pair_sum(p, r, yp, HC, HC).astype(BF16)
        s_m[r, pl.ds(0, HC)] = pair_sum(p, r, ym, 0, HC).astype(BF16)
        arrived((p, r, 1), own.at[0, rows(r)], to_yp)
        s_p[r, pl.ds(0, HC)] = (pair_sum(p, r, yp, 0, HC) + r_a[r].astype(F32)).astype(BF16)
        send(("ring", p), (p, r, 2), s_p.at[r], r_p.at[r], to_yp)
        s_m[r, pl.ds(HC, HC)] = (pair_sum(p, r, ym, HC, HC) + r_b[r].astype(F32)).astype(BF16)
        send(("ring", p), (p, r, 2), s_m.at[r], r_m.at[r], to_ym)

    odd = lax.rem(x, 2)
    column = {1: 1 - odd, 2: odd}

    def s3(p, r):
        own, r_p, r_m = sums[p][0], sums[p][9], sums[p][10]
        total = pair_sum(p, r, y, 0, CH)
        arrived((p, r, 2), own.at[pl.ds(0, 2), rows(r)], to_yp)
        total = total + (r_p[r].astype(F32) + r_m[r].astype(F32))
        if p == 0:
            mg[me, rows(r), :] = (xg[me, rows(r), :].astype(F32) + total).astype(BF16)
            return
        mixed = mg[me, rows(r), :]
        mixed = jnp.where(column[p] == 0, mixed[:, :128], mixed[:, 128:]).astype(F32)
        columns = pl.ds(pl.multiple_of(column[p] * 128, 128), 128)
        out[rows(r), columns] = (mixed + total).astype(BF16)

    def norm(src, gain, r):
        def body(i, carry):
            at = pl.ds(pl.multiple_of(r * CH + i * 64, 64), 64)
            square = jnp.zeros((64, DV), F32)
            for b in range(8):
                v = src[b, at, :].astype(F32)
                square = square + v * v
            mean = jnp.sum(square, axis=-1, keepdims=True) * (1.0 / D)
            scale = lax.rsqrt(mean + EPS)
            for b in range(8):
                v = src[b, at, :].astype(F32)
                g = gain[pl.ds(b * DV, DV)].reshape(1, DV).astype(F32)
                nrm[at, b * DV : (b + 1) * DV] = (v * scale * g).astype(BF16)
            return carry

        lax.fori_loop(0, CH // 64, body, 0, unroll=2)

    def dot(a, b):
        return jnp.dot(a, b, preferred_element_type=F32)

    def mixa(r):
        a = nrm[rows(r), :]
        qkv = dot(a, wq[:, :, :, 0 : 2 * DK + DV].reshape(D, 2 * DK + DV))
        q = qkv[:, :DK].astype(BF16)
        kbuf[rows(r), :] = qkv[:, DK : 2 * DK].astype(BF16)
        vbuf[rows(r), :] = qkv[:, 2 * DK :].astype(BF16)
        gate = dot(a, wq[:, :, :, 2 * DK + DV :].reshape(D, DV))
        kept = jnp.zeros((CH, DV), F32)
        for b in range(r + 1):
            score = lax.dot_general(
                q, kbuf[rows(b), :], (((1,), (1,)), ((), ())), preferred_element_type=F32
            )
            score = (score * dec[r - b]).astype(BF16)
            kept = kept + dot(score, vbuf[rows(b), :])
        mean = jnp.mean(kept * kept, axis=-1, keepdims=True)
        kept = kept * lax.rsqrt(mean + EPS)
        hid[rows(r), :] = (gate / (1.0 + jnp.exp(-gate)) * kept).astype(BF16)

    def mix(r):
        own, snd = sums[0][:2]
        for dst, cc in ((snd, other), (own, c)):
            for b in range(4):
                right = jnp.concatenate([wo[b, 2 * cc], wo[b, 2 * cc + 1]], axis=1)
                dst[b, rows(r), :] = dot(hid[rows(r), :], right).astype(BF16)
            if dst is snd:
                s0(0, r)

    def up(r):
        a = nrm[rows(r), :]
        for b in range(4):
            upward = dot(a, wu[:, :, :, b * 256 : (b + 1) * 256].reshape(D, 256))
            upward = jnp.maximum(upward, 0.0)
            act[rows(r), b * 256 : (b + 1) * 256] = (upward * upward).astype(BF16)

    def down(p, r):
        own, snd = sums[p][:2]
        for dst, cc in ((snd, other), (own, c)):
            for b in (0, 2):
                at = 2 * cc + column[p]
                right = jnp.concatenate([wd[b, at], wd[b + 1, at]], axis=1)
                value = dot(act[rows(r), :], right).astype(BF16)
                dst[b, rows(r), :] = value[:, :128]
                dst[b + 1, rows(r), :] = value[:, 128:]
            if dst is snd:
                s0(p, r)

    def load(names):
        own = (xg.at[me], wq_own, wo.at[zl, x], wu.at[zl, x], wd.at[zl, x], gmix, gmlp)
        for i, ref in enumerate(own):
            if "tqoudab"[i] in names:
                pltpu.make_async_copy(ref, ref, local_sem.at[i]).wait()

    feats = {"t": (xg, gmix), "m": (mg, gmlp)}
    kinds = {"w3": w3, "w4": w4, "w5": w5}
    plain = {
        "load": load, "w1": w1, "w2": w2, "s1": s1, "s2": s2, "s3": s3,
        "mixa": mixa, "mix": mix, "up": up, "down": down,
    }
    gathers = {"g1": g1, "g2": g2, "g3": g3, "g4": g4}
    for name, *args in ORDER:
        if name == "norm":
            norm(*feats[args[0]], args[1])
        elif name in gathers:
            gathers[name](args[0], feats[args[0]][0], args[1])
        elif name in plain:
            plain[name](*args)
        else:
            kinds[name[:2]](name[2], *args)
    def left(out_group, whole):
        remote(out_group, next(iter(arrivals)), whole, whole, to_pair).wait_send()

    for w, (buf, _) in weights.items():
        left((w, "first"), shards(w, 3))
        left((w, "third"), buf.at[pl.ds(0, 2)])
        left((w, "fourth"), shards(w, 4))
    for tag, (buf, _) in feats.items():
        left(tag, buf.at[pl.ds(0, 7)])
    for p in range(3):
        own = sums[p][0]
        left(("pair", p), own)
        left(("ring", p), own.at[pl.ds(0, 3)])


def local(
    tokens, gain_mix, query_weight, key_weight, value_weight, gate_weight,
    decay_rate, out_weight, gain_mlp, up_weight, down_weight,
):
    hbm = pl.BlockSpec(memory_space=pltpu.HBM)
    vmem = pl.BlockSpec(memory_space=pltpu.VMEM)
    smem = pl.BlockSpec(memory_space=pltpu.SMEM)

    def summing(width):
        whole = [pltpu.VMEM((4, SEQ, width), BF16)] * 3
        moved = [pltpu.VMEM((NCH, n, width), BF16) for n in (HC, HC, CH, CH)]
        return whole + moved + moved

    def stay(v):
        return pltpu.with_memory_space_constraint(v, pltpu.HBM)

    return pl.pallas_call(
        kernel,
        out_shape=jax.ShapeDtypeStruct((SEQ, DV), BF16),
        in_specs=[hbm, hbm, hbm, hbm, hbm, hbm, smem, hbm, hbm, hbm, hbm],
        out_specs=vmem,
        scratch_shapes=[
            pltpu.VMEM((D,), BF16),
            pltpu.VMEM((D,), BF16),
            pltpu.VMEM((8, SEQ, DV), BF16),
            pltpu.VMEM((8, SEQ, DV), BF16),
            pltpu.VMEM((SEQ, D), BF16),
            pltpu.VMEM((4, 4, 128, 768), BF16),
            pltpu.VMEM((4, 4, 256, 128), BF16),
            pltpu.VMEM((4, 4, 128, 1024), BF16),
            pltpu.VMEM((4, 4, 1024, 128), BF16),
            pltpu.VMEM((SEQ, DK), BF16),
            pltpu.VMEM((SEQ, DV), BF16),
            pltpu.VMEM((NCH, CH, CH), F32),
            pltpu.VMEM((SEQ, DV), BF16),
            pltpu.VMEM((SEQ, 1024), BF16),
            pltpu.SemaphoreType.DMA((N_SENDS,)),
            pltpu.SemaphoreType.DMA((N_ARRIVALS,)),
            pltpu.SemaphoreType.DMA((N_LOCAL,)),
            *summing(DV), *summing(128), *summing(128),
        ],
        compiler_params=pltpu.CompilerParams(
            collective_id=0, has_side_effects=True, vmem_limit_bytes=52 * 1024 * 1024
        ),
    )(
        stay(tokens), stay(gain_mix), stay(query_weight), stay(key_weight), stay(value_weight),
        stay(gate_weight), decay_rate, stay(out_weight), stay(gain_mlp), stay(up_weight),
        stay(down_weight),
    )


def solution(mesh):
    finer = Mesh(
        mesh.devices.reshape(mesh.shape["rep"], 4, 4, 4, 2), ("rep", "zl", "x", "y", "c")
    )
    placed = (
        P(("rep", "zl", "x"), TP), P(), P(FS, TP), P(FS, TP), P(FS, TP), P(FS, TP),
        P(TP), P(TP, FS), P(), P(FS, TP), P(TP, FS),
    )
    return jax.shard_map(
        local, mesh=finer, in_specs=placed, out_specs=P(("rep", "zl", "x"), TP), check_vma=False
    )
```
